512 devices in a mesh: fs: 64 (over z, y), tp: 8 (over x, core).
Axes of the slice: x: 4, y: 4, z: 16, core: 2. Of those that a mesh axis runs over, the one named last changes fastest.
Arguments:
- fwd_tokens: bfloat16 [8192, 2048], P('fs'), may hold values from -6 to 6
- back_tokens: bfloat16 [8192, 2048], P('fs'), may hold values from -16 to 16
- out_grad: bfloat16 [8192, 2048], P('fs'), may hold values from -16 to 16
- norm_gain: float32 [2048], replicated, may hold values from 0.1 to 1.9
- gate_weight: bfloat16 [2048, 2816], P('fs', 'tp'), may hold values from -0.125 to 0.125
- up_weight: bfloat16 [2048, 2816], P('fs', 'tp'), may hold values from -0.125 to 0.125
- down_weight: bfloat16 [2048, 2816], P('fs', 'tp'), may hold values from -0.109375 to 0.109375
- gate_grad_sum: float32 [2048, 2816], P('fs', 'tp'), may hold values from -96 to 96
Outputs:
- fwd_out: bfloat16 [8192, 2048], P('fs')
- back_grad: bfloat16 [8192, 2048], P('fs')
- gate_grad_out: float32 [2048, 2816], P('fs', 'tp')
The draws below stay inside these ranges and needn't reach their ends.
All inputs are finite; a program needn't handle non-finite values.
Results may differ from the reference program's by a relative error of at most 0.014.
Values may be sent and summed in bfloat16 or wider, within the bound.
No kernel may reach another device: no remote copies, remote signals or barrier semaphores. Data moves between devices by JAX's collectives and lax.ppermute only.
A program may use at most 64 MiB of HBM per device.

```python
import jax
import jax.numpy as jnp
from jax import lax

D = 2048
FF = 2816
TOKENS = 8192
N_TP = 8


def spiked(entries, own_key, source, target, parts, factor):
    def block_of(dim):
        return (jnp.arange(entries.shape[dim]) // (entries.shape[dim] // parts)).reshape((-1,) + (1,) * (entries.ndim - 1 - dim))

    near = jax.random.permutation(own_key, parts)[block_of(target)]
    far = (block_of(target) + parts // 2) % parts
    return jnp.where((block_of(source) == near) | (block_of(source) == far), factor * entries, entries)


def level_of(key, shape, pieces, smallest, high):
    def one(position, blocks):
        draws = jax.random.uniform(jax.random.fold_in(jax.random.fold_in(key, 6), position), (blocks,), jnp.float32, smallest / len(pieces), high / len(pieces))
        return jnp.repeat(jnp.exp(draws), shape[position] // blocks).reshape((-1,) + (1,) * (len(shape) - position - 1))

    gain = one(*pieces[0])
    for cut in pieces[1:]:
        gain = gain * one(*cut)
    return gain


def scatter_about(own_key, shape, spread, bound, split=(), kind=jnp.bfloat16):
    entries = spread * jax.random.normal(own_key, shape, jnp.float32)
    if split:
        entries = entries * level_of(own_key, shape, split, -0.22, 0.18)
    return jnp.clip(entries, -bound, bound).astype(kind)


def noise_with(key, shape, width, most, split, heavy, kind=jnp.bfloat16):
    drawn = width * jax.random.normal(key, shape, jnp.float32)
    if split:
        drawn = drawn * level_of(key, shape, split, -0.22, 0.18)
    return jnp.clip(spiked(drawn, jax.random.fold_in(key, 3), *heavy), -most, most).astype(kind)


def setup_inputs(seed: int = 0) -> dict:
    streams_of = jax.random.split(jax.random.key(seed), 9)
    return {
        "fwd_tokens": scatter_about(streams_of[0], (TOKENS, D), 1.0, 6.0, ((0, 64),)),
        "back_tokens": noise_with(streams_of[1], (TOKENS, D), 1.0, 16.0, ((0, 64),), (0, 1, 64, 4.0)),
        "out_grad": noise_with(streams_of[2], (TOKENS, D), 1.0, 16.0, ((0, 64),), (0, 1, 64, 4.0)),
        "norm_gain": jnp.clip(1.0 + 0.18 * jax.random.normal(streams_of[3], (D,), jnp.float32), 0.1, 1.9),
        "gate_weight": scatter_about(streams_of[4], (D, FF), D ** -0.5, 0.125, ((0, 64), (1, 8))),
        "up_weight": scatter_about(streams_of[5], (D, FF), D ** -0.5, 0.125, ((0, 64), (1, 8))),
        "down_weight": scatter_about(streams_of[6], (D, FF), FF ** -0.5, 0.109375, ((0, 64), (1, 8))),
        "gate_grad_sum": scatter_about(streams_of[7], (D, FF), 16.0, 96.0, ((0, 64), (1, 8)), jnp.float32),
    }


norm_eps = 0.25

def normalize(tokens, norm_gain):
    values = tokens.astype(jnp.float32)
    factor = lax.rsqrt(lax.optimization_barrier(jnp.mean(values * values, axis=-1, keepdims=True)) + norm_eps)
    return (values, factor, (values * factor * norm_gain).astype(jnp.bfloat16))

def rounded(block_part):
    return lax.optimization_barrier(block_part.astype(jnp.bfloat16)).astype(jnp.float32)

def reference(fwd_tokens, back_tokens, out_grad, norm_gain, gate_weight, up_weight, down_weight, gate_grad_sum):
    col_width = FF // N_TP
    fwd_normed = normalize(fwd_tokens, norm_gain)[2]
    gate_pre = jnp.dot(fwd_normed, gate_weight, preferred_element_type=jnp.float32)
    up_pre = jnp.dot(fwd_normed, up_weight, preferred_element_type=jnp.float32)
    hidden = (gate_pre * jax.nn.sigmoid(gate_pre) * up_pre).astype(jnp.bfloat16)
    summed = jnp.zeros((TOKENS, D), jnp.float32)
    for tp_block in range(N_TP):
        lower = tp_block * col_width
        upper = lower + col_width
        block_part = jnp.dot(hidden[:, lower:upper], down_weight[:, lower:upper].T, preferred_element_type=jnp.float32)
        summed = summed + rounded(block_part)
    fwd_out = (0.5 * summed).astype(jnp.bfloat16)
    values, factor, back_normed = normalize(back_tokens, norm_gain)
    gate_pre = jnp.dot(back_normed, gate_weight, preferred_element_type=jnp.float32)
    up_pre = jnp.dot(back_normed, up_weight, preferred_element_type=jnp.float32)
    sigmoid_gate = jax.nn.sigmoid(gate_pre)
    back_hidden = 0.5 * jnp.dot(out_grad, down_weight, preferred_element_type=jnp.float32)
    gate_diff = (back_hidden * up_pre * sigmoid_gate * (1.0 + gate_pre * (1.0 - sigmoid_gate))).astype(jnp.bfloat16)
    up_diff = (back_hidden * gate_pre * sigmoid_gate).astype(jnp.bfloat16)
    normed_diff = jnp.zeros((TOKENS, D), jnp.float32)
    for tp_block in range(N_TP):
        lower = tp_block * col_width
        upper = lower + col_width
        block_part = jnp.dot(gate_diff[:, lower:upper], gate_weight[:, lower:upper].T, preferred_element_type=jnp.float32)
        block_part = block_part + jnp.dot(up_diff[:, lower:upper], up_weight[:, lower:upper].T, preferred_element_type=jnp.float32)
        normed_diff = normed_diff + rounded(block_part)
    scaled = normed_diff * norm_gain
    cubed = factor * factor * factor
    back_grad = (factor * scaled - values * cubed * lax.optimization_barrier(jnp.mean(scaled * values, axis=-1, keepdims=True))).astype(jnp.bfloat16)
    gate_grad_out = gate_grad_sum + jnp.dot(back_normed.T, gate_diff, preferred_element_type=jnp.float32)
    return (fwd_out, back_grad, gate_grad_out)
```

```python
import jax
import jax.numpy as jnp
from jax import lax
from jax.experimental import pallas as pl
from jax.experimental.pallas import tpu as pltpu
from jax.sharding import Mesh
from jax.sharding import PartitionSpec as P

Z = ("za", "zb")
FS = ("za", "zb", "y")
TP = ("x", "c")
norm_eps = 0.25
F32 = jnp.float32
BF = jnp.bfloat16


def shift(array, axis, by):
    n = lax.axis_size(axis)
    return lax.ppermute(array, axis, [(k, (k + by) % n) for k in range(n)])


def copies_to_all(array, axis):
    copies = jnp.broadcast_to(array, (lax.axis_size(axis), *array.shape))
    return lax.all_to_all(copies, axis, split_axis=0, concat_axis=0, tiled=True)


def normalize(tokens, gain):
    values = tokens.astype(F32)
    factor = lax.rsqrt(jnp.mean(values * values, axis=-1, keepdims=True) + norm_eps)
    return (values * factor * gain).astype(BF)


def dot(a, b, ca, cb):
    return lax.dot_general(a, b, (((ca,), (cb,)), ((), ())), preferred_element_type=F32)


def products(at, ft, bt, og, gain, s0, s1, s2a, s2b, s3, parts, grads, wg, wu, wd, full):
    zb, y = at[0], at[1]
    for dy, pieces in ((0, (s0,)), (1, (s1,)), (2, (s2a, s2b)), (3, (s3,))):
        b = 0
        for piece in pieces:
            for k in range(piece.shape[0]):
                r, za = b // 4, b % 4
                row = za * 512 + ((zb + r) % 4) * 128 + ((y + dy) % 4) * 32
                rows = pl.ds(pl.multiple_of(row, 32), 32)
                for m, whole in enumerate((wg, wu, wd)):
                    whole[rows, :] = piece[k, m * 32 : (m + 1) * 32, :]
                b += 1
    g = gain[...]
    bn = normalize(bt[...], g)
    gate = dot(bn, wg[...], 1, 0)
    up = dot(bn, wu[...], 1, 0)
    hid = 0.5 * dot(og[...], wd[...], 1, 0)
    s = jax.nn.sigmoid(gate)
    gd = (hid * up * s * (1.0 + gate * (1.0 - s))).astype(BF)
    ud = (hid * gate * s).astype(BF)
    full[...] = dot(bn, gd, 0, 0).astype(BF)
    for dy in range(4):
        for z in range(16):
            row = z * 128 + ((y + dy) % 4) * 32
            grads[dy, z * 32 : (z + 1) * 32, :] = full[pl.ds(pl.multiple_of(row, 32), 32), :]
    diff = dot(gd, wg[...], 1, 1) + dot(ud, wu[...], 1, 1)
    diff = diff.astype(BF)
    fn = normalize(ft[...], g)
    gate = dot(fn, wg[...], 1, 0)
    up = dot(fn, wu[...], 1, 0)
    hidden = (gate * jax.nn.sigmoid(gate) * up).astype(BF)
    out = dot(hidden, wd[...], 1, 1).astype(BF)
    for x in range(4):
        for c in range(2):
            t = (c * 4 + x) * 16
            parts[x * 2 + c, :, 0:2048] = out[t : t + 16, :]
            parts[x * 2 + c, :, 2048:4096] = diff[t : t + 16, :]


def finish(at, recv, bt, gain, out):
    rows = pl.ds(pl.multiple_of(at[0] * 16, 16), 16)
    total = recv[0].astype(F32)
    for k in range(1, 8):
        total = total + recv[k].astype(F32)
    out[:, 0:2048] = (0.5 * total[:, 0:2048]).astype(BF)
    values = bt[rows, :].astype(F32)
    factor = lax.rsqrt(jnp.mean(values * values, axis=-1, keepdims=True) + norm_eps)
    scaled = total[:, 2048:4096] * gain[...]
    cubed = factor * factor * factor
    mean = jnp.mean(scaled * values, axis=-1, keepdims=True)
    out[:, 2048:4096] = (factor * scaled - values * cubed * mean).astype(BF)


VM = pl.BlockSpec(memory_space=pltpu.VMEM)
SM = pl.BlockSpec(memory_space=pltpu.SMEM)


def shards(ft, bt, og, gain, gw, uw, dw, gsum):
    zb, y = lax.axis_index("zb"), lax.axis_index("y")
    x, c = lax.axis_index("x"), lax.axis_index("c")
    gain = gain.reshape(1, 2048)
    own = jnp.concatenate([gw, uw, dw], axis=0)
    r0 = copies_to_all(own, "za")
    r1 = shift(r0, Z, -1)
    r3 = shift(r0, Z, 1)
    r2a = shift(r1[:2], Z, -1)
    r2b = shift(r3[2:], Z, 1)
    s0 = jnp.concatenate([r0, r1, r2a, r2b, r3], axis=0)
    s1 = shift(s0, "y", -1)
    s3 = shift(s0, "y", 1)
    s2a = shift(s1[:8], "y", -1)
    s2b = shift(s3[8:], "y", 1)
    at = jnp.stack([zb, y]).astype(jnp.int32)
    parts, grads = pl.pallas_call(
        products,
        name="products",
        out_shape=(
            jax.ShapeDtypeStruct((8, 16, 4096), BF),
            jax.ShapeDtypeStruct((4, 512, 352), BF),
        ),
        in_specs=[SM] + [VM] * 9,
        out_specs=(VM, VM),
        scratch_shapes=[pltpu.VMEM((2048, 352), BF)] * 4,
    )(at, ft, bt, og, gain, s0, s1, s2a, s2b, s3)
    g1 = shift(grads[1], "y", 1)
    g3 = shift(grads[3], "y", -1)
    g2 = shift(grads[2], "y", 2)
    recv = lax.all_to_all(parts, TP, split_axis=0, concat_axis=0, tiled=True)
    gy = grads[0].astype(F32) + g1.astype(F32) + g2.astype(F32) + g3.astype(F32)
    gz = lax.all_to_all(
        gy.astype(BF).reshape(16, 32, 352), Z, split_axis=0, concat_axis=0, tiled=True
    )
    done = pl.pallas_call(
        finish,
        name="finish",
        out_shape=jax.ShapeDtypeStruct((16, 4096), BF),
        in_specs=[SM] + [VM] * 3,
        out_specs=VM,
    )((c * 4 + x).astype(jnp.int32).reshape(1), recv, bt, gain)
    half = lax.all_gather(done, "x", axis=0, tiled=True)
    other = shift(half, "c", 1)
    first = jnp.where(c == 0, half, other)
    second = jnp.where(c == 0, other, half)
    whole = jnp.concatenate([first, second], axis=0)
    grad = gsum + gz.astype(F32).sum(axis=0)
    return whole[:, :2048], whole[:, 2048:], grad


def solution(mesh):
    split = Mesh(mesh.devices.reshape(4, 4, 4, 4, 2), ("za", "zb", "y", "x", "c"))
    tok = P(FS, None)
    w = P(FS, TP)
    return jax.shard_map(
        shards,
        mesh=split,
        in_specs=(tok, tok, tok, P(), w, w, w, w),
        out_specs=(tok, tok, w),
        check_vma=False,
    )
```

```python
import jax
import jax.numpy as jnp
from jax import lax
from jax.experimental import pallas as pl
from jax.experimental.pallas import tpu as pltpu
from jax.sharding import Mesh
from jax.sharding import PartitionSpec as P

Z = ("za", "zb")
FS = ("za", "zb", "y")
TP = ("x", "c")
norm_eps = 0.25
F32 = jnp.float32
BF = jnp.bfloat16


def shift(array, axis, by):
    n = lax.axis_size(axis)
    return lax.ppermute(array, axis, [(k, (k + by) % n) for k in range(n)])


def copies_to_all(array, axis):
    copies = jnp.broadcast_to(array, (lax.axis_size(axis), *array.shape))
    return lax.all_to_all(copies, axis, split_axis=0, concat_axis=0, tiled=True)


def normalize(tokens, gain):
    values = tokens.astype(F32)
    factor = lax.rsqrt(jnp.mean(values * values, axis=-1, keepdims=True) + norm_eps)
    return (values * factor * gain).astype(BF)


def dot(a, b, ca, cb):
    return lax.dot_general(a, b, (((ca,), (cb,)), ((), ())), preferred_element_type=F32)


PIECES = (
    ((0, 4, 0, 0, 0),),
    ((0, 4, 1, 0, 0),),
    ((0, 4, 3, 0, 0),),
    ((0, 4, 0, 1, 0),),
    ((0, 4, 0, 3, 0),),
    ((0, 4, 1, 1, 0), (4, 6, 2, 0, 0)),
    ((0, 4, 3, 3, 0), (4, 6, 2, 0, 2)),
    ((0, 4, 3, 1, 0), (4, 6, 0, 2, 0)),
    ((0, 4, 1, 3, 0), (4, 6, 0, 2, 2)),
    ((0, 4, 1, 2, 0),),
    ((0, 4, 3, 2, 0),),
    ((0, 4, 2, 1, 0),),
    ((0, 4, 2, 3, 0),),
    ((0, 2, 2, 2, 0),),
    ((0, 2, 2, 2, 2),),
)


def products(at, ft, bt, og, gain, *refs):
    pieces, (parts, grads, wg, wu, wd, full) = refs[: len(PIECES)], refs[len(PIECES) :]
    zb, y = at[0], at[1]
    for piece, spans in zip(pieces, PIECES):
        for lo, hi, r, dy, za0 in spans:
            base = ((zb + r) % 4) * 128 + ((y + dy) % 4) * 32
            for k in range(lo, hi):
                rows = pl.ds(pl.multiple_of((za0 + k - lo) * 512 + base, 32), 32)
                for m, whole in enumerate((wg, wu, wd)):
                    whole[rows, :] = piece[k, m * 32 : (m + 1) * 32, :]
    g = gain[...]
    bn = normalize(bt[...], g)
    gate = dot(bn, wg[...], 1, 0)
    up = dot(bn, wu[...], 1, 0)
    hid = 0.5 * dot(og[...], wd[...], 1, 0)
    s = jax.nn.sigmoid(gate)
    gd = (hid * up * s * (1.0 + gate * (1.0 - s))).astype(BF)
    ud = (hid * gate * s).astype(BF)
    full[...] = dot(bn, gd, 0, 0).astype(BF)
    for dy in range(4):
        for z in range(16):
            row = z * 128 + ((y + dy) % 4) * 32
            grads[dy, z * 32 : (z + 1) * 32, :] = full[pl.ds(pl.multiple_of(row, 32), 32), :]
    diff = dot(gd, wg[...], 1, 1) + dot(ud, wu[...], 1, 1)
    diff = diff.astype(BF)
    fn = normalize(ft[...], g)
    gate = dot(fn, wg[...], 1, 0)
    up = dot(fn, wu[...], 1, 0)
    hidden = (gate * jax.nn.sigmoid(gate) * up).astype(BF)
    out = dot(hidden, wd[...], 1, 1).astype(BF)
    for x in range(4):
        for c in range(2):
            t = (c * 4 + x) * 16
            parts[x * 2 + c, :, 0:2048] = out[t : t + 16, :]
            parts[x * 2 + c, :, 2048:4096] = diff[t : t + 16, :]


def finish(at, recv, bt, gain, out):
    rows = pl.ds(pl.multiple_of(at[0] * 16, 16), 16)
    total = recv[0].astype(F32)
    for k in range(1, 8):
        total = total + recv[k].astype(F32)
    out[:, 0:2048] = (0.5 * total[:, 0:2048]).astype(BF)
    values = bt[rows, :].astype(F32)
    factor = lax.rsqrt(jnp.mean(values * values, axis=-1, keepdims=True) + norm_eps)
    scaled = total[:, 2048:4096] * gain[...]
    cubed = factor * factor * factor
    mean = jnp.mean(scaled * values, axis=-1, keepdims=True)
    out[:, 2048:4096] = (factor * scaled - values * cubed * mean).astype(BF)


VM = pl.BlockSpec(memory_space=pltpu.VMEM)
SM = pl.BlockSpec(memory_space=pltpu.SMEM)


def shards(ft, bt, og, gain, gw, uw, dw, gsum):
    zb, y = lax.axis_index("zb"), lax.axis_index("y")
    x, c = lax.axis_index("x"), lax.axis_index("c")
    gain = gain.reshape(1, 2048)
    own = jnp.concatenate([gw, uw, dw], axis=0)
    a = copies_to_all(own, "za")
    a1, a3 = shift(a, Z, -1), shift(a, Z, 1)
    b1, b3 = shift(a, "y", -1), shift(a, "y", 1)
    c1 = shift(jnp.concatenate([b1, a1[:2]]), Z, -1)
    c3 = shift(jnp.concatenate([b3, a3[2:]]), Z, 1)
    d1 = shift(jnp.concatenate([a3, b1[:2]]), "y", -1)
    d3 = shift(jnp.concatenate([a1, b3[2:]]), "y", 1)
    far_y = jnp.concatenate([d1[4:], d3[4:]])
    far_z = jnp.concatenate([c1[4:], c3[4:]])
    e1, e3 = shift(far_y, Z, -1), shift(far_y, Z, 1)
    f1, f3 = shift(far_z, "y", -1), shift(far_z, "y", 1)
    h1, h3 = shift(d1[4:], Z, -2), shift(d3[4:], Z, 2)
    pieces = (a, a1, a3, b1, b3, c1, c3, d1, d3, e1, e3, f1, f3, h1, h3)
    at = jnp.stack([zb, y]).astype(jnp.int32)
    parts, grads = pl.pallas_call(
        products,
        name="products",
        out_shape=(
            jax.ShapeDtypeStruct((8, 16, 4096), BF),
            jax.ShapeDtypeStruct((4, 512, 352), BF),
        ),
        in_specs=[SM] + [VM] * (4 + len(PIECES)),
        out_specs=(VM, VM),
        scratch_shapes=[pltpu.VMEM((2048, 352), BF)] * 4,
    )(at, ft, bt, og, gain, *pieces)
    g1 = shift(grads[1], "y", 1)
    g3 = shift(grads[3], "y", -1)
    g2 = shift(grads[2], "y", 2)
    recv = lax.all_to_all(parts, TP, split_axis=0, concat_axis=0, tiled=True)
    gy = grads[0].astype(F32) + g1.astype(F32) + g2.astype(F32) + g3.astype(F32)
    gy, recv = lax.optimization_barrier((gy.astype(BF), recv))
    gz = lax.all_to_all(
        gy.reshape(16, 32, 352), Z, split_axis=0, concat_axis=0, tiled=True
    )
    done = pl.pallas_call(
        finish,
        name="finish",
        out_shape=jax.ShapeDtypeStruct((16, 4096), BF),
        in_specs=[SM] + [VM] * 3,
        out_specs=VM,
    )((c * 4 + x).astype(jnp.int32).reshape(1), recv, bt, gain)
    half = lax.all_gather(done, "x", axis=0, tiled=True)
    other = shift(half, "c", 1)
    first = jnp.where(c == 0, half, other)
    second = jnp.where(c == 0, other, half)
    whole = jnp.concatenate([first, second], axis=0)
    grad = gsum + gz.astype(F32).sum(axis=0)
    return whole[:, :2048], whole[:, 2048:], grad


def solution(mesh):
    split = Mesh(mesh.devices.reshape(4, 4, 4, 4, 2), ("za", "zb", "y", "x", "c"))
    tok = P(FS, None)
    w = P(FS, TP)
    return jax.shard_map(
        shards,
        mesh=split,
        in_specs=(tok, tok, tok, P(), w, w, w, w),
        out_specs=(tok, tok, w),
        check_vma=False,
    )
```

```python
import jax
import jax.numpy as jnp
from jax import lax
from jax.experimental import pallas as pl
from jax.experimental.pallas import tpu as pltpu
from jax.sharding import Mesh
from jax.sharding import PartitionSpec as P

Z = ("za", "zb")
FS = ("za", "zb", "y")
TP = ("x", "c")
norm_eps = 0.25
F32 = jnp.float32
BF = jnp.bfloat16


def shift(array, axis, by):
    n = lax.axis_size(axis)
    return lax.ppermute(array, axis, [(k, (k + by) % n) for k in range(n)])


def copies_to_all(array, axis):
    copies = jnp.broadcast_to(array, (lax.axis_size(axis), *array.shape))
    return lax.all_to_all(copies, axis, split_axis=0, concat_axis=0, tiled=True)


def normalize(tokens, gain):
    values = tokens.astype(F32)
    factor = lax.rsqrt(jnp.mean(values * values, axis=-1, keepdims=True) + norm_eps)
    return (values * factor * gain).astype(BF)


def dot(a, b, ca, cb):
    return lax.dot_general(a, b, (((ca,), (cb,)), ((), ())), preferred_element_type=F32)


def assemble(at, pieces, wholes):
    zb, y = at[0], at[1]
    near, a1, a3, far, z1, z3 = pieces
    todo = []
    for yy in range(4):
        for za in range(4):
            todo.append((near, (yy, za), za * 512 + zb * 128 + yy * 32))
            todo.append((far, (yy, za), za * 512 + (zb + 2) % 4 * 128 + yy * 32))
    for r, mine, other in ((1, a1, z1), (3, a3, z3)):
        base = (zb + r) % 4 * 128
        for za in range(4):
            todo.append((mine, (za,), za * 512 + base + y * 32))
            for dy in range(1, 4):
                todo.append((other, (dy - 1, za), za * 512 + base + (y + dy) % 4 * 32))
    for piece, spot, row in todo:
        rows = pl.ds(pl.multiple_of(row, 32), 32)
        for m, whole in enumerate(wholes):
            whole[rows, :] = piece[(*spot, slice(m * 32, (m + 1) * 32))]


def prepare(at, bt, ft, og, gain, bn, fn, oc):
    bn[...] = normalize(bt[...], gain[...])
    fn[...] = normalize(ft[...], gain[...])
    oc[...] = og[...]


def backward(at, bn, og, *refs):
    pieces, (grads, gd_out, ud_out, wg, wu, wd) = refs[:6], refs[6:]
    assemble(at, pieces, (wg, wu, wd))
    gate = dot(bn[...], wg[...], 1, 0)
    up = dot(bn[...], wu[...], 1, 0)
    hid = 0.5 * dot(og[...], wd[...], 1, 0)
    s = jax.nn.sigmoid(gate)
    gd = (hid * up * s * (1.0 + gate * (1.0 - s))).astype(BF)
    gd_out[...] = gd
    ud_out[...] = (hid * gate * s).astype(BF)
    part = dot(bn[...], gd, 0, 0).astype(BF)
    for yy in range(4):
        for z in range(16):
            row = (z * 4 + yy) * 32
            grads[yy, z, :, :] = part[row : row + 32, :]


def rest(at, fn, gd, ud, *refs):
    pieces, (keep, give, wg, wu, wd, parts) = refs[:6], refs[6:]
    assemble(at, pieces, (wg, wu, wd))
    diff = dot(gd[...], wg[...], 1, 1) + dot(ud[...], wu[...], 1, 1)
    parts[:, 2048:4096] = diff.astype(BF)
    gate = dot(fn[...], wg[...], 1, 0)
    up = dot(fn[...], wu[...], 1, 0)
    hidden = (gate * jax.nn.sigmoid(gate) * up).astype(BF)
    parts[:, 0:2048] = dot(hidden, wd[...], 1, 1).astype(BF)
    c = at[2]
    keep[...] = parts[pl.ds(pl.multiple_of(c * 64, 64), 64), :]
    give[...] = parts[pl.ds(pl.multiple_of((1 - c) * 64, 64), 64), :]


def pair(at, keep, other, *outs):
    for k, out in enumerate(outs):
        rows = pl.ds(pl.multiple_of((at[3] + k) % 4 * 16, 16), 16)
        out[...] = (keep[rows, :].astype(F32) + other[rows, :].astype(F32)).astype(BF)


def finish(at, p0, p1, p2, p3, bt, gain, out):
    rows = pl.ds(pl.multiple_of((at[2] * 4 + at[3]) * 16, 16), 16)
    total = p0[...].astype(F32) + p1[...].astype(F32) + p2[...].astype(F32) + p3[...].astype(F32)
    out[:, 0:2048] = (0.5 * total[:, 0:2048]).astype(BF)
    values = bt[rows, :].astype(F32)
    factor = lax.rsqrt(jnp.mean(values * values, axis=-1, keepdims=True) + norm_eps)
    scaled = total[:, 2048:4096] * gain[...]
    cubed = factor * factor * factor
    mean = jnp.mean(scaled * values, axis=-1, keepdims=True)
    out[:, 2048:4096] = (factor * scaled - values * cubed * mean).astype(BF)


VM = pl.BlockSpec(memory_space=pltpu.VMEM)
SM = pl.BlockSpec(memory_space=pltpu.SMEM)


def call(body, outs, scratch, *args):
    return pl.pallas_call(
        body,
        out_shape=tuple(jax.ShapeDtypeStruct(o, BF) for o in outs),
        in_specs=[SM] + [VM] * (len(args) - 1),
        out_specs=(VM,) * len(outs),
        scratch_shapes=[pltpu.VMEM(o, BF) for o in scratch],
        compiler_params=pltpu.CompilerParams(vmem_limit_bytes=LIMIT),
    )(*args)


LIMIT = 24 * 1024 * 1024
W = (2048, 352)
TOK = (128, 2048)
HID = (128, 352)


def exchange(array, axis):
    return lax.all_to_all(array, axis, split_axis=0, concat_axis=0, tiled=True)


def shards(ft, bt, og, gain, gw, uw, dw, gsum):
    spots = [lax.axis_index(n) for n in ("zb", "y", "c", "x")]
    y, c = spots[1], spots[2]
    at = jnp.stack(spots).astype(jnp.int32)
    gain = gain.reshape(1, 2048)
    own = jnp.concatenate([gw, uw, dw], axis=0)
    a = copies_to_all(own, "za")
    near = copies_to_all(a, "y")
    a1 = shift(a, Z, -1)
    a3 = shift(a, Z, 1)
    a2 = jnp.concatenate([shift(a[:2], Z, -2), shift(a[2:], Z, 2)])
    others = lax.dynamic_slice_in_dim(jnp.concatenate([near, near]), y + 1, 3)
    z1 = shift(others, Z, -1)
    z3 = shift(others, Z, 1)
    far = copies_to_all(a2, "y")
    pieces = (near, a1, a3, far, z1, z3)
    bn, fn, oc = call(prepare, (TOK,) * 3, (), at, bt, ft, og, gain)
    grads, gd, ud = call(backward, ((4, 16, 32, 352), HID, HID), (W,) * 3, at, bn, oc, *pieces)
    gy = exchange(grads, "y")
    keep, give = call(rest, ((64, 4096),) * 2, (W, W, W, (128, 4096)), at, fn, gd, ud, *pieces)
    other = shift(give, "c", 1)
    p0, p1, p2, p3 = call(pair, ((16, 4096),) * 4, (), at, keep, other)
    p1, p2, p3 = shift(p1, "x", 1), shift(p2, "x", 2), shift(p3, "x", -1)
    gy = gy.astype(F32).sum(axis=0).astype(BF)
    gz = exchange(gy, Z)
    (done,) = call(finish, ((16, 4096),), (), at, p0, p1, p2, p3, bt, gain)
    half = lax.all_gather(done, "x", axis=0, tiled=True)
    other = shift(half, "c", 1)
    first = jnp.where(c == 0, half, other)
    second = jnp.where(c == 0, other, half)
    whole = jnp.concatenate([first, second], axis=0)
    grad = gsum + gz.astype(F32).sum(axis=0)
    return whole[:, :2048], whole[:, 2048:], grad


def solution(mesh):
    split = Mesh(mesh.devices.reshape(4, 4, 4, 4, 2), ("za", "zb", "y", "x", "c"))
    tok = P(FS, None)
    w = P(FS, TP)
    return jax.shard_map(
        shards,
        mesh=split,
        in_specs=(tok, tok, tok, P(), w, w, w, w),
        out_specs=(tok, tok, w),
        check_vma=False,
    )
```

```python
import jax
import jax.numpy as jnp
from jax import lax
from jax.experimental import pallas as pl
from jax.experimental.pallas import tpu as pltpu
from jax.sharding import Mesh
from jax.sharding import PartitionSpec as P

Z = ("za", "zb")
FS = ("za", "zb", "y")
TP = ("x", "c")
norm_eps = 0.25
F32 = jnp.float32
BF = jnp.bfloat16


def shift(array, axis, by):
    n = lax.axis_size(axis)
    return lax.ppermute(array, axis, [(k, (k + by) % n) for k in range(n)])


def copies_to_all(array, axis):
    copies = jnp.broadcast_to(array, (lax.axis_size(axis), *array.shape))
    return lax.all_to_all(copies, axis, split_axis=0, concat_axis=0, tiled=True)


def normalize(tokens, gain):
    values = tokens.astype(F32)
    factor = lax.rsqrt(jnp.mean(values * values, axis=-1, keepdims=True) + norm_eps)
    return (values * factor * gain).astype(BF)


def dot(a, b, ca, cb):
    return lax.dot_general(a, b, (((ca,), (cb,)), ((), ())), preferred_element_type=F32)


def assemble(at, pieces, wholes):
    zb, y = at[0], at[1]
    near, a1, a3, far, z1, z3 = pieces
    todo = []
    for yy in range(4):
        for za in range(4):
            todo.append((near, (yy, za), za * 512 + zb * 128 + yy * 32))
            todo.append((far, (yy, za), za * 512 + (zb + 2) % 4 * 128 + yy * 32))
    for r, mine, other in ((1, a1, z1), (3, a3, z3)):
        base = (zb + r) % 4 * 128
        for za in range(4):
            todo.append((mine, (za,), za * 512 + base + y * 32))
            for dy in range(1, 4):
                todo.append((other, (dy - 1, za), za * 512 + base + (y + dy) % 4 * 32))
    for piece, spot, row in todo:
        rows = pl.ds(pl.multiple_of(row, 32), 32)
        for m, whole in enumerate(wholes):
            whole[rows, :] = piece[(*spot, slice(m * 32, (m + 1) * 32))]


def prepare(at, bt, ft, og, gain, bo, fn, b0, b1, b2, b3, split):
    y = at[1]
    fn[...] = normalize(ft[...], gain[...])
    normed = normalize(bt[...], gain[...])
    bo[0] = normed
    bo[1] = og[...]
    tiles = [normed[:, z * 128 : (z + 1) * 128].astype(F32) for z in range(16)]
    spot = lax.broadcasted_iota(jnp.int32, (128, 128), 1) // 32
    for yy in range(4):
        for q in range(4):
            tile = tiles[4 * q]
            for j in range(4):
                moved = tiles[4 * q + j]
                if j != yy:
                    moved = pltpu.roll(moved, (j - yy) % 4 * 32, 1)
                tile = jnp.where(spot == j, moved, tile)
            split[yy, :, q * 128 : (q + 1) * 128] = tile.astype(BF)
    for k, out in enumerate((b0, b1, b2, b3)):
        out[...] = split[(y + k) % 4]


def backward(at, bo, *refs):
    pieces, (gds, both, wg, wu, wd) = refs[:6], refs[6:]
    assemble(at, pieces, (wg, wu, wd))
    gate = dot(bo[0], wg[...], 1, 0)
    up = dot(bo[0], wu[...], 1, 0)
    hid = 0.5 * dot(bo[1], wd[...], 1, 0)
    s = jax.nn.sigmoid(gate)
    gd = (hid * up * s * (1.0 + gate * (1.0 - s))).astype(BF)
    for k in range(4):
        for j in range(4):
            gds[k, j] = gd[j * 32 : (j + 1) * 32, :]
    both[0] = gd
    both[1] = (hid * gate * s).astype(BF)


def outer(at, b0, b1, b2, b3, gds, grads):
    y = at[1]
    total = dot(b0[...], gds[y].reshape(128, 352), 0, 0)
    for k, piece in ((1, b1), (2, b2), (3, b3)):
        total = total + dot(piece[...], gds[(y + 4 - k) % 4].reshape(128, 352), 0, 0)
    total = total.astype(BF)
    for z in range(16):
        grads[z] = total[z * 32 : (z + 1) * 32, :]


def rest(at, fn, both, *refs):
    pieces, (keep, give, wg, wu, wd, parts) = refs[:6], refs[6:]
    assemble(at, pieces, (wg, wu, wd))
    diff = dot(both[0], wg[...], 1, 1) + dot(both[1], wu[...], 1, 1)
    parts[:, 2048:4096] = diff.astype(BF)
    gate = dot(fn[...], wg[...], 1, 0)
    up = dot(fn[...], wu[...], 1, 0)
    hidden = (gate * jax.nn.sigmoid(gate) * up).astype(BF)
    parts[:, 0:2048] = dot(hidden, wd[...], 1, 1).astype(BF)
    c = at[2]
    keep[...] = parts[pl.ds(pl.multiple_of(c * 64, 64), 64), :]
    give[...] = parts[pl.ds(pl.multiple_of((1 - c) * 64, 64), 64), :]


def pair(at, keep, other, *outs):
    for k, out in enumerate(outs):
        rows = pl.ds(pl.multiple_of((at[3] + k) % 4 * 16, 16), 16)
        out[...] = (keep[rows, :].astype(F32) + other[rows, :].astype(F32)).astype(BF)


def finish(at, p0, p1, p2, p3, bt, gain, out):
    rows = pl.ds(pl.multiple_of((at[2] * 4 + at[3]) * 16, 16), 16)
    total = p0[...].astype(F32) + p1[...].astype(F32) + p2[...].astype(F32) + p3[...].astype(F32)
    out[:, 0:2048] = (0.5 * total[:, 0:2048]).astype(BF)
    values = bt[rows, :].astype(F32)
    factor = lax.rsqrt(jnp.mean(values * values, axis=-1, keepdims=True) + norm_eps)
    scaled = total[:, 2048:4096] * gain[...]
    cubed = factor * factor * factor
    mean = jnp.mean(scaled * values, axis=-1, keepdims=True)
    out[:, 2048:4096] = (factor * scaled - values * cubed * mean).astype(BF)


VM = pl.BlockSpec(memory_space=pltpu.VMEM)
SM = pl.BlockSpec(memory_space=pltpu.SMEM)


def call(body, outs, scratch, *args):
    return pl.pallas_call(
        body,
        out_shape=tuple(jax.ShapeDtypeStruct(o, BF) for o in outs),
        in_specs=[SM] + [VM] * (len(args) - 1),
        out_specs=(VM,) * len(outs),
        scratch_shapes=[pltpu.VMEM(o, BF) for o in scratch],
        compiler_params=pltpu.CompilerParams(vmem_limit_bytes=LIMIT),
    )(*args)


LIMIT = 24 * 1024 * 1024
W = (2048, 352)
TOK = (128, 2048)
HID = (128, 352)
COL = (128, 512)


def exchange(array, axis):
    return lax.all_to_all(array, axis, split_axis=0, concat_axis=0, tiled=True)


def shards(ft, bt, og, gain, gw, uw, dw, gsum):
    spots = [lax.axis_index(n) for n in ("zb", "y", "c", "x")]
    y, c = spots[1], spots[2]
    at = jnp.stack(spots).astype(jnp.int32)
    gain = gain.reshape(1, 2048)
    own = jnp.concatenate([gw, uw, dw], axis=0)
    a = copies_to_all(own, "za")
    near = copies_to_all(a, "y")
    a1 = shift(a, Z, -1)
    a3 = shift(a, Z, 1)
    a2 = jnp.concatenate([shift(a[:2], Z, -2), shift(a[2:], Z, 2)])
    others = lax.dynamic_slice_in_dim(jnp.concatenate([near, near]), y + 1, 3)
    z1 = shift(others, Z, -1)
    z3 = shift(others, Z, 1)
    far = copies_to_all(a2, "y")
    pieces = (near, a1, a3, far, z1, z3)
    bo, fn, b0, b1, b2, b3 = call(
        prepare, ((2, *TOK), TOK) + (COL,) * 4, ((4, *COL),), at, bt, ft, og, gain
    )
    b1 = shift(b1, "y", 1)
    b2 = shift(b2, "y", 2)
    b3 = shift(b3, "y", 3)
    gds, both = call(backward, ((4, 4, 32, 352), (2, *HID)), (W,) * 3, at, bo, *pieces)
    gds = exchange(gds, "y")
    keep, give = call(rest, ((64, 4096),) * 2, (W, W, W, (128, 4096)), at, fn, both, *pieces)
    (grads,) = call(outer, ((16, 32, 352),), (), at, b0, b1, b2, b3, gds)
    gz = exchange(grads, Z)
    other = shift(give, "c", 1)
    p0, p1, p2, p3 = call(pair, ((16, 4096),) * 4, (), at, keep, other)
    p1, p2, p3 = shift(p1, "x", 1), shift(p2, "x", 2), shift(p3, "x", -1)
    (done,) = call(finish, ((16, 4096),), (), at, p0, p1, p2, p3, bt, gain)
    half = lax.all_gather(done, "x", axis=0, tiled=True)
    other = shift(half, "c", 1)
    first = jnp.where(c == 0, half, other)
    second = jnp.where(c == 0, other, half)
    whole = jnp.concatenate([first, second], axis=0)
    grad = gsum + gz.astype(F32).sum(axis=0)
    return whole[:, :2048], whole[:, 2048:], grad


def solution(mesh):
    split = Mesh(mesh.devices.reshape(4, 4, 4, 4, 2), ("za", "zb", "y", "x", "c"))
    tok = P(FS, None)
    w = P(FS, TP)
    return jax.shard_map(
        shards,
        mesh=split,
        in_specs=(tok, tok, tok, P(), w, w, w, w),
        out_specs=(tok, tok, w),
        check_vma=False,
    )
```

```python
import jax
import jax.numpy as jnp
from jax import lax
from jax.experimental import pallas as pl
from jax.experimental.pallas import tpu as pltpu
from jax.sharding import Mesh
from jax.sharding import PartitionSpec as P

Z = ("za", "zb")
FS = ("za", "zb", "y")
TP = ("x", "c")
norm_eps = 0.25
F32 = jnp.float32
BF = jnp.bfloat16


def shift(array, axis, by):
    n = lax.axis_size(axis)
    return lax.ppermute(array, axis, [(k, (k + by) % n) for k in range(n)])


def copies_to_all(array, axis):
    copies = jnp.broadcast_to(array, (lax.axis_size(axis), *array.shape))
    return lax.all_to_all(copies, axis, split_axis=0, concat_axis=0, tiled=True)


def normalize(tokens, gain):
    values = tokens.astype(F32)
    factor = lax.rsqrt(jnp.mean(values * values, axis=-1, keepdims=True) + norm_eps)
    return (values * factor * gain).astype(BF)


def dot(a, b, ca, cb):
    return lax.dot_general(a, b, (((ca,), (cb,)), ((), ())), preferred_element_type=F32)


def assemble(at, pieces, wholes):
    zb, y = at[0], at[1]
    near, a1, a3, far, z1, z3 = pieces
    todo = []
    for yy in range(4):
        for za in range(4):
            todo.append((near, (yy, za), za * 512 + zb * 128 + yy * 32))
            todo.append((far, (yy, za), za * 512 + (zb + 2) % 4 * 128 + yy * 32))
    for r, mine, other in ((1, a1, z1), (3, a3, z3)):
        base = (zb + r) % 4 * 128
        for za in range(4):
            todo.append((mine, (za,), za * 512 + base + y * 32))
            for dy in range(1, 4):
                todo.append((other, (dy - 1, za), za * 512 + base + (y + dy) % 4 * 32))
    for piece, spot, row in todo:
        rows = pl.ds(pl.multiple_of(row, 32), 32)
        for m, whole in enumerate(wholes):
            whole[rows, :] = piece[(*spot, slice(m * 32, (m + 1) * 32))]


def prepare(at, bt, ft, og, gain, bo, fn, b0, b1, b2, b3, split):
    y = at[1]
    fn[...] = normalize(ft[...], gain[...])
    normed = normalize(bt[...], gain[...])
    bo[0] = normed
    bo[1] = og[...]
    tiles = [normed[:, z * 128 : (z + 1) * 128].astype(F32) for z in range(16)]
    spot = lax.broadcasted_iota(jnp.int32, (128, 128), 1) // 32
    for yy in range(4):
        for q in range(4):
            tile = tiles[4 * q]
            for j in range(4):
                moved = tiles[4 * q + j]
                if j != yy:
                    moved = pltpu.roll(moved, (j - yy) % 4 * 32, 1)
                tile = jnp.where(spot == j, moved, tile)
            split[yy, :, q * 128 : (q + 1) * 128] = tile.astype(BF)
    for k, out in enumerate((b0, b1, b2, b3)):
        out[...] = split[(y + k) % 4]


def backward(at, bo, *refs):
    pieces, (gds, both, wg, wu, wd) = refs[:6], refs[6:]
    assemble(at, pieces, (wg, wu, wd))
    gate = dot(bo[0], wg[...], 1, 0)
    up = dot(bo[0], wu[...], 1, 0)
    hid = 0.5 * dot(bo[1], wd[...], 1, 0)
    s = jax.nn.sigmoid(gate)
    gd = (hid * up * s * (1.0 + gate * (1.0 - s))).astype(BF)
    for k in range(4):
        for j in range(4):
            gds[k, j] = gd[j * 32 : (j + 1) * 32, :]
    both[0] = gd
    both[1] = (hid * gate * s).astype(BF)


def merge(at, b0, b1, b2, b3, out):
    for k, piece in enumerate((b0, b1, b2, b3)):
        out[(at[1] + 4 - k) % 4] = piece[...]


def outer(at, columns, gds, grads):
    total = dot(columns[0], gds[0].reshape(128, 352), 0, 0)
    for k in range(1, 4):
        total = total + dot(columns[k], gds[k].reshape(128, 352), 0, 0)
    total = total.astype(BF)
    for z in range(16):
        grads[z] = total[z * 32 : (z + 1) * 32, :]


def rest(at, fn, both, *refs):
    pieces, (keep, give, wg, wu, wd, parts) = refs[:6], refs[6:]
    assemble(at, pieces, (wg, wu, wd))
    diff = dot(both[0], wg[...], 1, 1) + dot(both[1], wu[...], 1, 1)
    parts[:, 2048:4096] = diff.astype(BF)
    gate = dot(fn[...], wg[...], 1, 0)
    up = dot(fn[...], wu[...], 1, 0)
    hidden = (gate * jax.nn.sigmoid(gate) * up).astype(BF)
    parts[:, 0:2048] = dot(hidden, wd[...], 1, 1).astype(BF)
    c = at[2]
    keep[...] = parts[pl.ds(pl.multiple_of(c * 64, 64), 64), :]
    give[...] = parts[pl.ds(pl.multiple_of((1 - c) * 64, 64), 64), :]


def pair(at, keep, other, *outs):
    for k, out in enumerate(outs):
        rows = pl.ds(pl.multiple_of((at[3] + k) % 4 * 16, 16), 16)
        out[...] = (keep[rows, :].astype(F32) + other[rows, :].astype(F32)).astype(BF)


def finish(at, p0, p1, p2, p3, bt, gain, out):
    rows = pl.ds(pl.multiple_of((at[2] * 4 + at[3]) * 16, 16), 16)
    total = p0[...].astype(F32) + p1[...].astype(F32) + p2[...].astype(F32) + p3[...].astype(F32)
    out[:, 0:2048] = (0.5 * total[:, 0:2048]).astype(BF)
    values = bt[rows, :].astype(F32)
    factor = lax.rsqrt(jnp.mean(values * values, axis=-1, keepdims=True) + norm_eps)
    scaled = total[:, 2048:4096] * gain[...]
    cubed = factor * factor * factor
    mean = jnp.mean(scaled * values, axis=-1, keepdims=True)
    out[:, 2048:4096] = (factor * scaled - values * cubed * mean).astype(BF)


VM = pl.BlockSpec(memory_space=pltpu.VMEM)
SM = pl.BlockSpec(memory_space=pltpu.SMEM)


def call(body, outs, scratch, *args):
    return pl.pallas_call(
        body,
        out_shape=tuple(jax.ShapeDtypeStruct(o, BF) for o in outs),
        in_specs=[SM] + [VM] * (len(args) - 1),
        out_specs=(VM,) * len(outs),
        scratch_shapes=[pltpu.VMEM(o, BF) for o in scratch],
        compiler_params=pltpu.CompilerParams(vmem_limit_bytes=LIMIT),
    )(*args)


LIMIT = 24 * 1024 * 1024
W = (2048, 352)
TOK = (128, 2048)
HID = (128, 352)
COL = (128, 512)


def exchange(array, axis):
    return lax.all_to_all(array, axis, split_axis=0, concat_axis=0, tiled=True)


def shards(ft, bt, og, gain, gw, uw, dw, gsum):
    spots = [lax.axis_index(n) for n in ("zb", "y", "c", "x")]
    y, c = spots[1], spots[2]
    at = jnp.stack(spots).astype(jnp.int32)
    gain = gain.reshape(1, 2048)
    own = jnp.concatenate([gw, uw, dw], axis=0)
    a = copies_to_all(own, "za")
    near = copies_to_all(a, "y")
    a1 = shift(a, Z, -1)
    a3 = shift(a, Z, 1)
    a2 = jnp.concatenate([shift(a[:2], Z, -2), shift(a[2:], Z, 2)])
    others = lax.dynamic_slice_in_dim(jnp.concatenate([near, near]), y + 1, 3)
    z1 = shift(others, Z, -1)
    z3 = shift(others, Z, 1)
    far = copies_to_all(a2, "y")
    pieces = (near, a1, a3, far, z1, z3)
    bo, fn, b0, b1, b2, b3 = call(
        prepare, ((2, *TOK), TOK) + (COL,) * 4, ((4, *COL),), at, bt, ft, og, gain
    )
    b1 = shift(b1, "y", 1)
    b2 = shift(b2, "y", 2)
    b3 = shift(b3, "y", 3)
    (columns,) = call(merge, ((4, *COL),), (), at, b0, b1, b2, b3)
    gds, both = call(backward, ((4, 4, 32, 352), (2, *HID)), (W,) * 3, at, bo, *pieces)
    gds = exchange(gds, "y")
    keep, give = call(rest, ((64, 4096),) * 2, (W, W, W, (128, 4096)), at, fn, both, *pieces)
    (grads,) = call(outer, ((16, 32, 352),), (), at, columns, gds)
    gz = exchange(grads, Z)
    other = shift(give, "c", 1)
    p0, p1, p2, p3 = call(pair, ((16, 4096),) * 4, (), at, keep, other)
    p1, p2, p3 = shift(p1, "x", 1), shift(p2, "x", 2), shift(p3, "x", -1)
    (done,) = call(finish, ((16, 4096),), (), at, p0, p1, p2, p3, bt, gain)
    half = lax.all_gather(done, "x", axis=0, tiled=True)
    other = shift(half, "c", 1)
    first = jnp.where(c == 0, half, other)
    second = jnp.where(c == 0, other, half)
    whole = jnp.concatenate([first, second], axis=0)
    grad = gsum + gz.astype(F32).sum(axis=0)
    return whole[:, :2048], whole[:, 2048:], grad


def solution(mesh):
    split = Mesh(mesh.devices.reshape(4, 4, 4, 4, 2), ("za", "zb", "y", "x", "c"))
    tok = P(FS, None)
    w = P(FS, TP)
    return jax.shard_map(
        shards,
        mesh=split,
        in_specs=(tok, tok, tok, P(), w, w, w, w),
        out_specs=(tok, tok, w),
        check_vma=False,
    )
```

```python
import jax
import jax.numpy as jnp
from jax import lax
from jax.experimental import pallas as pl
from jax.experimental.pallas import tpu as pltpu
from jax.sharding import Mesh
from jax.sharding import PartitionSpec as P

Z = ("za", "zb")
FS = ("za", "zb", "y")
TP = ("x", "c")
norm_eps = 0.25
F32 = jnp.float32
BF = jnp.bfloat16


def shift(array, axis, by):
    n = lax.axis_size(axis)
    return lax.ppermute(array, axis, [(k, (k + by) % n) for k in range(n)])


def copies_to_all(array, axis):
    copies = jnp.broadcast_to(array, (lax.axis_size(axis), *array.shape))
    return lax.all_to_all(copies, axis, split_axis=0, concat_axis=0, tiled=True)


def normalize(tokens, gain):
    values = tokens.astype(F32)
    factor = lax.rsqrt(jnp.mean(values * values, axis=-1, keepdims=True) + norm_eps)
    return (values * factor * gain).astype(BF)


def dot(a, b, ca, cb):
    return lax.dot_general(a, b, (((ca,), (cb,)), ((), ())), preferred_element_type=F32)


def assemble(at, pieces, wholes):
    zb, y = at[0], at[1]
    near, a1, a3, far, z1, z3 = pieces
    todo = []
    for yy in range(4):
        for za in range(4):
            todo.append((near, (yy, za), za * 512 + zb * 128 + yy * 32))
            todo.append((far, (yy, za), za * 512 + (zb + 2) % 4 * 128 + yy * 32))
    for r, mine, other in ((1, a1, z1), (3, a3, z3)):
        base = (zb + r) % 4 * 128
        for za in range(4):
            todo.append((mine, (za,), za * 512 + base + y * 32))
            for dy in range(1, 4):
                todo.append((other, (dy - 1, za), za * 512 + base + (y + dy) % 4 * 32))
    for piece, spot, row in todo:
        rows = pl.ds(pl.multiple_of(row, 32), 32)
        for m, whole in enumerate(wholes):
            whole[rows, :] = piece[(*spot, slice(m * 32, (m + 1) * 32))]


def columns(at, bt, gain, b0, b1, b2, b3, split):
    y = at[1]
    normed = normalize(bt[...], gain[...])
    tiles = [normed[:, z * 128 : (z + 1) * 128].astype(F32) for z in range(16)]
    spot = lax.broadcasted_iota(jnp.int32, (128, 128), 1) // 32
    for yy in range(4):
        for q in range(4):
            tile = tiles[4 * q]
            for j in range(4):
                moved = tiles[4 * q + j]
                if j != yy:
                    moved = pltpu.roll(moved, (j - yy) % 4 * 32, 1)
                tile = jnp.where(spot == j, moved, tile)
            split[yy, :, q * 128 : (q + 1) * 128] = tile.astype(BF)
    for k, out in enumerate((b0, b1, b2, b3)):
        out[...] = split[(y + k) % 4]


def tokens(at, bt, ft, og, gain, out):
    out[0] = normalize(bt[...], gain[...])
    out[1] = og[...]
    out[2] = normalize(ft[...], gain[...])


def products(at, tok, *refs):
    pieces, (gds, keep, give, wg, wu, wd, parts) = refs[:6], refs[6:]
    assemble(at, pieces, (wg, wu, wd))
    gate = dot(tok[0], wg[...], 1, 0)
    up = dot(tok[0], wu[...], 1, 0)
    hid = 0.5 * dot(tok[1], wd[...], 1, 0)
    s = jax.nn.sigmoid(gate)
    gd = (hid * up * s * (1.0 + gate * (1.0 - s))).astype(BF)
    ud = (hid * gate * s).astype(BF)
    for k in range(4):
        for j in range(4):
            gds[k, j] = gd[j * 32 : (j + 1) * 32, :]
    parts[:, 2048:4096] = (dot(gd, wg[...], 1, 1) + dot(ud, wu[...], 1, 1)).astype(BF)
    gate = dot(tok[2], wg[...], 1, 0)
    up = dot(tok[2], wu[...], 1, 0)
    hidden = (gate * jax.nn.sigmoid(gate) * up).astype(BF)
    parts[:, 0:2048] = dot(hidden, wd[...], 1, 1).astype(BF)
    c = at[2]
    keep[...] = parts[pl.ds(pl.multiple_of(c * 64, 64), 64), :]
    give[...] = parts[pl.ds(pl.multiple_of((1 - c) * 64, 64), 64), :]


def merge(at, b0, b1, b2, b3, out):
    for k, piece in enumerate((b0, b1, b2, b3)):
        out[(at[1] + 4 - k) % 4] = piece[...]


def outer(at, cols, gds, grads):
    total = dot(cols[0], gds[0].reshape(128, 352), 0, 0)
    for k in range(1, 4):
        total = total + dot(cols[k], gds[k].reshape(128, 352), 0, 0)
    total = total.astype(BF)
    for z in range(16):
        grads[z] = total[z * 32 : (z + 1) * 32, :]


def pair(at, keep, other, *outs):
    for k, out in enumerate(outs):
        rows = pl.ds(pl.multiple_of((at[3] + k) % 4 * 16, 16), 16)
        out[...] = (keep[rows, :].astype(F32) + other[rows, :].astype(F32)).astype(BF)


def finish(at, p0, p1, p2, p3, bt, gain, out):
    rows = pl.ds(pl.multiple_of((at[2] * 4 + at[3]) * 16, 16), 16)
    total = p0[...].astype(F32) + p1[...].astype(F32) + p2[...].astype(F32) + p3[...].astype(F32)
    out[:, 0:2048] = (0.5 * total[:, 0:2048]).astype(BF)
    values = bt[rows, :].astype(F32)
    factor = lax.rsqrt(jnp.mean(values * values, axis=-1, keepdims=True) + norm_eps)
    scaled = total[:, 2048:4096] * gain[...]
    cubed = factor * factor * factor
    mean = jnp.mean(scaled * values, axis=-1, keepdims=True)
    out[:, 2048:4096] = (factor * scaled - values * cubed * mean).astype(BF)


VM = pl.BlockSpec(memory_space=pltpu.VMEM)
SM = pl.BlockSpec(memory_space=pltpu.SMEM)


def call(body, outs, scratch, *args):
    return pl.pallas_call(
        body,
        out_shape=tuple(jax.ShapeDtypeStruct(o, BF) for o in outs),
        in_specs=[SM] + [VM] * (len(args) - 1),
        out_specs=(VM,) * len(outs),
        scratch_shapes=[pltpu.VMEM(o, BF) for o in scratch],
        compiler_params=pltpu.CompilerParams(vmem_limit_bytes=LIMIT),
    )(*args)


LIMIT = 24 * 1024 * 1024
W = (2048, 352)
TOK = (128, 2048)
COL = (128, 512)


def exchange(array, axis):
    return lax.all_to_all(array, axis, split_axis=0, concat_axis=0, tiled=True)


def shards(ft, bt, og, gain, gw, uw, dw, gsum):
    spots = [lax.axis_index(n) for n in ("zb", "y", "c", "x")]
    y, c = spots[1], spots[2]
    at = jnp.stack(spots).astype(jnp.int32)
    gain = gain.reshape(1, 2048)
    own = jnp.concatenate([gw, uw, dw], axis=0)
    a = copies_to_all(own, "za")
    near = copies_to_all(a, "y")
    a1 = shift(a, Z, -1)
    a3 = shift(a, Z, 1)
    a2 = jnp.concatenate([shift(a[:2], Z, -2), shift(a[2:], Z, 2)])
    others = lax.dynamic_slice_in_dim(jnp.concatenate([near, near]), y + 1, 3)
    z1 = shift(others, Z, -1)
    z3 = shift(others, Z, 1)
    far = copies_to_all(a2, "y")
    pieces = (near, a1, a3, far, z1, z3)
    b0, b1, b2, b3 = call(columns, (COL,) * 4, ((4, *COL),), at, bt, gain)
    (tok,) = call(tokens, ((3, *TOK),), (), at, bt, ft, og, gain)
    b1 = shift(b1, "y", 1)
    b2 = shift(b2, "y", 2)
    b3 = shift(b3, "y", 3)
    (cols,) = call(merge, ((4, *COL),), (), at, b0, b1, b2, b3)
    gds, keep, give = call(
        products,
        ((4, 4, 32, 352), (64, 4096), (64, 4096)),
        (W, W, W, (128, 4096)),
        at, tok, *pieces,
    )
    gds = exchange(gds, "y")
    (grads,) = call(outer, ((16, 32, 352),), (), at, cols, gds)
    gz = exchange(grads, Z)
    other = shift(give, "c", 1)
    p0, p1, p2, p3 = call(pair, ((16, 4096),) * 4, (), at, keep, other)
    p1, p2, p3 = shift(p1, "x", 1), shift(p2, "x", 2), shift(p3, "x", -1)
    (done,) = call(finish, ((16, 4096),), (), at, p0, p1, p2, p3, bt, gain)
    half = lax.all_gather(done, "x", axis=0, tiled=True)
    other = shift(half, "c", 1)
    first = jnp.where(c == 0, half, other)
    second = jnp.where(c == 0, other, half)
    whole = jnp.concatenate([first, second], axis=0)
    grad = gsum + gz.astype(F32).sum(axis=0)
    return whole[:, :2048], whole[:, 2048:], grad


def solution(mesh):
    split = Mesh(mesh.devices.reshape(4, 4, 4, 4, 2), ("za", "zb", "y", "x", "c"))
    tok = P(FS, None)
    w = P(FS, TP)
    return jax.shard_map(
        shards,
        mesh=split,
        in_specs=(tok, tok, tok, P(), w, w, w, w),
        out_specs=(tok, tok, w),
        check_vma=False,
    )
```

```python
import jax
import jax.numpy as jnp
from jax import lax
from jax.experimental import pallas as pl
from jax.experimental.pallas import tpu as pltpu
from jax.sharding import Mesh
from jax.sharding import PartitionSpec as P

Z = ("za", "zb")
FS = ("za", "zb", "y")
TP = ("x", "c")
norm_eps = 0.25
F32 = jnp.float32
BF = jnp.bfloat16


def shift(array, axis, by):
    n = lax.axis_size(axis)
    return lax.ppermute(array, axis, [(k, (k + by) % n) for k in range(n)])


def copies_to_all(array, axis):
    copies = jnp.broadcast_to(array, (lax.axis_size(axis), *array.shape))
    return lax.all_to_all(copies, axis, split_axis=0, concat_axis=0, tiled=True)


def normalize(tokens, gain):
    values = tokens.astype(F32)
    factor = lax.rsqrt(jnp.mean(values * values, axis=-1, keepdims=True) + norm_eps)
    return (values * factor * gain).astype(BF)


def dot(a, b, ca, cb):
    return lax.dot_general(a, b, (((ca,), (cb,)), ((), ())), preferred_element_type=F32)


def assemble(at, pieces, wholes, sems):
    zb, y = at[0], at[1]
    near, a1, a3, far, z1, z3 = pieces
    todo = []
    for yy in range(4):
        todo.append((near.at[yy], 0, yy))
        todo.append((far.at[yy], 2, yy))
    for r, mine, other in ((1, a1, z1), (3, a3, z3)):
        todo.append((mine, r, y))
        for dy in range(1, 4):
            todo.append((other.at[dy - 1], r, (y + dy) % 4))
    for m, whole in enumerate(wholes):
        for piece, r, yy in todo:
            pltpu.make_async_copy(
                piece.at[:, pl.ds(m * 32, 32), :], whole.at[:, (zb + r) % 4, yy], sems.at[m]
            ).start()


def columns(at, bt, gain, b0, b1, b2, b3, split):
    y = at[1]
    normed = normalize(bt[...], gain[...])
    tiles = [normed[:, z * 128 : (z + 1) * 128].astype(F32) for z in range(16)]
    spot = lax.broadcasted_iota(jnp.int32, (128, 128), 1) // 32
    for yy in range(4):
        for q in range(4):
            tile = tiles[4 * q]
            for j in range(4):
                moved = tiles[4 * q + j]
                if j != yy:
                    moved = pltpu.roll(moved, (j - yy) % 4 * 32, 1)
                tile = jnp.where(spot == j, moved, tile)
            split[yy, :, q * 128 : (q + 1) * 128] = tile.astype(BF)
    for k, out in enumerate((b0, b1, b2, b3)):
        out[...] = split[(y + k) % 4]


def tokens(at, bt, ft, og, gain, out):
    out[0] = normalize(bt[...], gain[...])
    out[1] = og[...]
    out[2] = normalize(ft[...], gain[...])


def products(at, tok, *refs):
    pieces, (gds, both, wg, wu, wd, parts, sems) = refs[:6], refs[6:]
    assemble(at, pieces, (wg, wu, wd), sems)
    ready = [False] * 3

    def weight(m):
        whole = (wg, wu, wd)[m]
        if not ready[m]:
            pltpu.make_async_copy(whole, whole, sems.at[m]).wait()
            ready[m] = True
        return whole[...].reshape(2048, 352)

    gate = dot(tok[0], weight(0), 1, 0)
    up = dot(tok[0], weight(1), 1, 0)
    hid = 0.5 * dot(tok[1], weight(2), 1, 0)
    s = jax.nn.sigmoid(gate)
    gd = (hid * up * s * (1.0 + gate * (1.0 - s))).astype(BF)
    ud = (hid * gate * s).astype(BF)
    for k in range(4):
        for j in range(4):
            gds[k, j] = gd[j * 32 : (j + 1) * 32, :]
    parts[:, 2048:4096] = (dot(gd, weight(0), 1, 1) + dot(ud, weight(1), 1, 1)).astype(BF)
    gate = dot(tok[2], weight(0), 1, 0)
    up = dot(tok[2], weight(1), 1, 0)
    hidden = (gate * jax.nn.sigmoid(gate) * up).astype(BF)
    parts[:, 0:2048] = dot(hidden, weight(2), 1, 1).astype(BF)
    c = at[2]
    both[0] = parts[pl.ds(pl.multiple_of(c * 64, 64), 64), :]
    both[1] = parts[pl.ds(pl.multiple_of((1 - c) * 64, 64), 64), :]


def merge(at, b0, b1, b2, b3, out):
    for k, piece in enumerate((b0, b1, b2, b3)):
        out[(at[1] + 4 - k) % 4] = piece[...]


def outer(at, cols, gds, grads):
    total = dot(cols[0], gds[0].reshape(128, 352), 0, 0)
    for k in range(1, 4):
        total = total + dot(cols[k], gds[k].reshape(128, 352), 0, 0)
    total = total.astype(BF)
    for z in range(16):
        grads[z] = total[z * 32 : (z + 1) * 32, :]


def pair(at, keep, other, *outs):
    for k, out in enumerate(outs):
        rows = pl.ds(pl.multiple_of((at[3] + k) % 4 * 16, 16), 16)
        out[...] = (keep[0, rows, :].astype(F32) + other[1, rows, :].astype(F32)).astype(BF)


def finish(at, p0, p1, p2, p3, bt, gain, out):
    rows = pl.ds(pl.multiple_of((at[2] * 4 + at[3]) * 16, 16), 16)
    total = p0[...].astype(F32) + p1[...].astype(F32) + p2[...].astype(F32) + p3[...].astype(F32)
    out[:, 0:2048] = (0.5 * total[:, 0:2048]).astype(BF)
    values = bt[rows, :].astype(F32)
    factor = lax.rsqrt(jnp.mean(values * values, axis=-1, keepdims=True) + norm_eps)
    scaled = total[:, 2048:4096] * gain[...]
    cubed = factor * factor * factor
    mean = jnp.mean(scaled * values, axis=-1, keepdims=True)
    out[:, 2048:4096] = (factor * scaled - values * cubed * mean).astype(BF)


VM = pl.BlockSpec(memory_space=pltpu.VMEM)
SM = pl.BlockSpec(memory_space=pltpu.SMEM)


def call(body, outs, scratch, *args, ins=None):
    return pl.pallas_call(
        body,
        out_shape=tuple(jax.ShapeDtypeStruct(o, BF) for o in outs),
        in_specs=[SM] + (ins or [VM] * (len(args) - 1)),
        out_specs=(VM,) * len(outs),
        scratch_shapes=[pltpu.VMEM(o, BF) if isinstance(o, tuple) else o for o in scratch],
        compiler_params=pltpu.CompilerParams(vmem_limit_bytes=LIMIT),
    )(*args)


LIMIT = 24 * 1024 * 1024
W = (4, 4, 4, 32, 352)
TOK = (128, 2048)
COL = (128, 512)


def exchange(array, axis):
    return lax.all_to_all(array, axis, split_axis=0, concat_axis=0, tiled=True)


def shards(ft, bt, og, gain, gw, uw, dw, gsum):
    spots = [lax.axis_index(n) for n in ("zb", "y", "c", "x")]
    y, c = spots[1], spots[2]
    at = jnp.stack(spots).astype(jnp.int32)
    gain = gain.reshape(1, 2048)
    own = jnp.concatenate([gw, uw, dw], axis=0)
    a = copies_to_all(own, "za")
    near = copies_to_all(a, "y")
    a1 = shift(a, Z, -1)
    a3 = shift(a, Z, 1)
    a2 = lax.ppermute(a, Z, [(k, (k + (2 if k % 2 else -2)) % 16) for k in range(16)])
    others = lax.dynamic_slice_in_dim(jnp.concatenate([near, near]), y + 1, 3)
    z1 = shift(others, Z, -1)
    z3 = shift(others, Z, 1)
    far = copies_to_all(a2, "y")
    pieces = (near, a1, a3, far, z1, z3)
    b0, b1, b2, b3 = call(columns, (COL,) * 4, ((4, *COL),), at, bt, gain)
    (tok,) = call(tokens, ((3, *TOK),), (), at, bt, ft, og, gain)
    b1 = shift(b1, "y", 1)
    b2 = shift(b2, "y", 2)
    b3 = shift(b3, "y", 3)
    (cols,) = call(merge, ((4, *COL),), (), at, b0, b1, b2, b3)
    gds, both = call(
        products,
        ((4, 4, 32, 352), (2, 64, 4096)),
        (W, W, W, (128, 4096), pltpu.SemaphoreType.DMA((3,))),
        at, tok, *pieces,
        ins=[VM] + [pl.BlockSpec(memory_space=pl.ANY)] * 6,
    )
    gds = exchange(gds, "y")
    (grads,) = call(outer, ((16, 32, 352),), (), at, cols, gds)
    gz = exchange(grads, Z)
    other = shift(both, "c", 1)
    p0, p1, p2, p3 = call(pair, ((16, 4096),) * 4, (), at, both, other)
    p1, p2, p3 = shift(p1, "x", 1), shift(p2, "x", 2), shift(p3, "x", -1)
    (done,) = call(finish, ((16, 4096),), (), at, p0, p1, p2, p3, bt, gain)
    half = lax.all_gather(done, "x", axis=0, tiled=True)
    other = shift(half, "c", 1)
    first = jnp.where(c == 0, half, other)
    second = jnp.where(c == 0, other, half)
    whole = jnp.concatenate([first, second], axis=0)
    grad = gsum + gz.astype(F32).sum(axis=0)
    return whole[:, :2048], whole[:, 2048:], grad


def solution(mesh):
    split = Mesh(mesh.devices.reshape(4, 4, 4, 4, 2), ("za", "zb", "y", "x", "c"))
    tok = P(FS, None)
    w = P(FS, TP)
    return jax.shard_map(
        shards,
        mesh=split,
        in_specs=(tok, tok, tok, P(), w, w, w, w),
        out_specs=(tok, tok, w),
        check_vma=False,
    )
```

```python
import jax
import jax.numpy as jnp
from jax import lax
from jax.experimental import pallas as pl
from jax.experimental.pallas import tpu as pltpu
from jax.sharding import Mesh
from jax.sharding import PartitionSpec as P

Z = ("za", "zb")
FS = ("za", "zb", "y")
TP = ("x", "c")
norm_eps = 0.25
F32 = jnp.float32
BF = jnp.bfloat16


def shift(array, axis, by):
    n = lax.axis_size(axis)
    return lax.ppermute(array, axis, [(k, (k + by) % n) for k in range(n)])


def copies_to_all(array, axis):
    copies = jnp.broadcast_to(array, (lax.axis_size(axis), *array.shape))
    return lax.all_to_all(copies, axis, split_axis=0, concat_axis=0, tiled=True)


def normalize(tokens, gain):
    values = tokens.astype(F32)
    factor = lax.rsqrt(jnp.mean(values * values, axis=-1, keepdims=True) + norm_eps)
    return (values * factor * gain).astype(BF)


def dot(a, b, ca, cb):
    return lax.dot_general(a, b, (((ca,), (cb,)), ((), ())), preferred_element_type=F32)


def assemble(at, pieces, wholes, sems):
    zb, y = at[0], at[1]
    near, a1, a3, far, z1, z3 = pieces
    todo = []
    for yy in range(4):
        todo.append((near.at[yy], 0, yy))
        todo.append((far.at[yy], 2, yy))
    for r, mine, other in ((1, a1, z1), (3, a3, z3)):
        todo.append((mine, r, y))
        for dy in range(1, 4):
            todo.append((other.at[dy - 1], r, (y + dy) % 4))
    for m, whole in enumerate(wholes):
        for piece, r, yy in todo:
            pltpu.make_async_copy(
                piece.at[:, pl.ds(m * 32, 32), :], whole.at[:, (zb + r) % 4, yy], sems.at[m]
            ).start()


def columns(at, bt, gain, b0, b1, b2, b3, split):
    y = at[1]
    normed = normalize(bt[...], gain[...])
    tiles = [normed[:, z * 128 : (z + 1) * 128].astype(F32) for z in range(16)]
    spot = lax.broadcasted_iota(jnp.int32, (128, 128), 1) // 32
    for yy in range(4):
        for q in range(4):
            tile = tiles[4 * q]
            for j in range(4):
                moved = tiles[4 * q + j]
                if j != yy:
                    moved = pltpu.roll(moved, (j - yy) % 4 * 32, 1)
                tile = jnp.where(spot == j, moved, tile)
            split[yy, :, q * 128 : (q + 1) * 128] = tile.astype(BF)
    for k, out in enumerate((b0, b1, b2, b3)):
        out[...] = split[(y + k) % 4]


def tokens(at, bt, ft, og, gain, out):
    out[0] = normalize(bt[...], gain[...])
    out[1] = og[...]
    out[2] = normalize(ft[...], gain[...])


def products(at, tok, *refs):
    pieces, (gds, both, wg, wu, wd, own, parts, sems, outs) = refs[:6], refs[6:]
    assemble(at, pieces, (wg, wu, wd), sems)
    ready = [False] * 3
    stores = []

    def weight(m):
        whole = (wg, wu, wd)[m]
        if not ready[m]:
            pltpu.make_async_copy(whole, whole, sems.at[m]).wait()
            ready[m] = True
        return whole[...].reshape(2048, 352)

    def store(source, target):
        copy = pltpu.make_async_copy(source, target, outs.at[len(stores)])
        copy.start()
        stores.append(copy)

    def store_parts(columns):
        for k, half in enumerate((at[2], 1 - at[2])):
            rows = pl.ds(pl.multiple_of(half * 64, 64), 64)
            store(parts.at[rows, columns], both.at[k, :, columns])

    gate = dot(tok[0], weight(0), 1, 0)
    up = dot(tok[0], weight(1), 1, 0)
    hid = 0.5 * dot(tok[1], weight(2), 1, 0)
    s = jax.nn.sigmoid(gate)
    gd = (hid * up * s * (1.0 + gate * (1.0 - s))).astype(BF)
    ud = (hid * gate * s).astype(BF)
    own[...] = gd.reshape(4, 32, 352)
    for k in range(4):
        store(own, gds.at[k])
    parts[:, 2048:4096] = (dot(gd, weight(0), 1, 1) + dot(ud, weight(1), 1, 1)).astype(BF)
    store_parts(pl.ds(2048, 2048))
    gate = dot(tok[2], weight(0), 1, 0)
    up = dot(tok[2], weight(1), 1, 0)
    hidden = (gate * jax.nn.sigmoid(gate) * up).astype(BF)
    parts[:, 0:2048] = dot(hidden, weight(2), 1, 1).astype(BF)
    store_parts(pl.ds(0, 2048))
    for copy in stores:
        copy.wait()


def merge(at, b0, b1, b2, b3, out):
    for k, piece in enumerate((b0, b1, b2, b3)):
        out[(at[1] + 4 - k) % 4] = piece[...]


def outer(at, cols, gds, grads):
    total = dot(cols[0], gds[0].reshape(128, 352), 0, 0)
    for k in range(1, 4):
        total = total + dot(cols[k], gds[k].reshape(128, 352), 0, 0)
    total = total.astype(BF)
    for z in range(16):
        grads[z] = total[z * 32 : (z + 1) * 32, :]


def pair(at, keep, other, *outs):
    for k, out in enumerate(outs):
        rows = pl.ds(pl.multiple_of((at[3] + k) % 4 * 16, 16), 16)
        out[...] = (keep[0, rows, :].astype(F32) + other[1, rows, :].astype(F32)).astype(BF)


def finish(at, p0, p1, p2, p3, bt, gain, out):
    rows = pl.ds(pl.multiple_of((at[2] * 4 + at[3]) * 16, 16), 16)
    total = p0[...].astype(F32) + p1[...].astype(F32) + p2[...].astype(F32) + p3[...].astype(F32)
    out[:, 0:2048] = (0.5 * total[:, 0:2048]).astype(BF)
    values = bt[rows, :].astype(F32)
    factor = lax.rsqrt(jnp.mean(values * values, axis=-1, keepdims=True) + norm_eps)
    scaled = total[:, 2048:4096] * gain[...]
    cubed = factor * factor * factor
    mean = jnp.mean(scaled * values, axis=-1, keepdims=True)
    out[:, 2048:4096] = (factor * scaled - values * cubed * mean).astype(BF)


VM = pl.BlockSpec(memory_space=pltpu.VMEM)
SM = pl.BlockSpec(memory_space=pltpu.SMEM)
ANY = pl.BlockSpec(memory_space=pl.ANY)
DMA = pltpu.SemaphoreType.DMA


def call(body, outs, scratch, *args, ins=None, to=None):
    shape = (lambda o: pltpu.HBM(o, BF)) if to else (lambda o: jax.ShapeDtypeStruct(o, BF))
    return pl.pallas_call(
        body,
        out_shape=tuple(shape(o) for o in outs),
        in_specs=[SM] + (ins or [VM] * (len(args) - 1)),
        out_specs=(to or VM,) * len(outs),
        scratch_shapes=[pltpu.VMEM(o, BF) if isinstance(o, tuple) else o for o in scratch],
        compiler_params=pltpu.CompilerParams(vmem_limit_bytes=LIMIT),
    )(*args)


LIMIT = 24 * 1024 * 1024
W = (4, 4, 4, 32, 352)
TOK = (128, 2048)
COL = (128, 512)


def exchange(array, axis):
    return lax.all_to_all(array, axis, split_axis=0, concat_axis=0, tiled=True)


def shards(ft, bt, og, gain, gw, uw, dw, gsum):
    spots = [lax.axis_index(n) for n in ("zb", "y", "c", "x")]
    y, c = spots[1], spots[2]
    at = jnp.stack(spots).astype(jnp.int32)
    gain = gain.reshape(1, 2048)
    own = jnp.concatenate([gw, uw, dw], axis=0)
    a = copies_to_all(own, "za")
    near = copies_to_all(a, "y")
    a1 = shift(a, Z, -1)
    a3 = shift(a, Z, 1)
    a2 = lax.ppermute(a, Z, [(k, (k + (2 if k % 2 else -2)) % 16) for k in range(16)])
    others = lax.dynamic_slice_in_dim(jnp.concatenate([near, near]), y + 1, 3)
    z1 = shift(others, Z, -1)
    z3 = shift(others, Z, 1)
    far = copies_to_all(a2, "y")
    pieces = (near, a1, a3, far, z1, z3)
    b0, b1, b2, b3 = call(columns, (COL,) * 4, ((4, *COL),), at, bt, gain)
    (tok,) = call(tokens, ((3, *TOK),), (), at, bt, ft, og, gain)
    b1 = shift(b1, "y", 1)
    b2 = shift(b2, "y", 2)
    b3 = shift(b3, "y", 3)
    (cols,) = call(merge, ((4, *COL),), (), at, b0, b1, b2, b3)
    gds, both = call(
        products,
        ((4, 4, 32, 352), (2, 64, 4096)),
        (W, W, W, (4, 32, 352), (128, 4096), DMA((3,)), DMA((8,))),
        at, tok, *pieces,
        ins=[VM] + [ANY] * 6,
        to=ANY,
    )
    gds = exchange(gds, "y")
    (grads,) = call(outer, ((16, 32, 352),), (), at, cols, gds)
    gz = exchange(grads, Z)
    other = shift(both, "c", 1)
    p0, p1, p2, p3 = call(pair, ((16, 4096),) * 4, (), at, both, other)
    p1 = shift(p1, "x", 1)
    p2 = shift(p2, "x", 2)
    p3 = shift(p3, "x", -1)
    (done,) = call(finish, ((16, 4096),), (), at, p0, p1, p2, p3, bt, gain)
    half = lax.all_gather(done, "x", axis=0, tiled=True)
    other = shift(half, "c", 1)
    first = jnp.where(c == 0, half, other)
    second = jnp.where(c == 0, other, half)
    whole = jnp.concatenate([first, second], axis=0)
    grad = gsum + gz.astype(F32).sum(axis=0)
    return whole[:, :2048], whole[:, 2048:], grad


def solution(mesh):
    split = Mesh(mesh.devices.reshape(4, 4, 4, 4, 2), ("za", "zb", "y", "x", "c"))
    tok = P(FS, None)
    w = P(FS, TP)
    return jax.shard_map(
        shards,
        mesh=split,
        in_specs=(tok, tok, tok, P(), w, w, w, w),
        out_specs=(tok, tok, w),
        check_vma=False,
    )
```

```python
import jax
import jax.numpy as jnp
from jax import lax
from jax.experimental import pallas as pl
from jax.experimental.pallas import tpu as pltpu
from jax.sharding import Mesh
from jax.sharding import PartitionSpec as P

Z = ("za", "zb")
FS = ("za", "zb", "y")
TP = ("x", "c")
norm_eps = 0.25
F32 = jnp.float32
BF = jnp.bfloat16


def shift(array, axis, by):
    n = lax.axis_size(axis)
    return lax.ppermute(array, axis, [(k, (k + by) % n) for k in range(n)])


def copies_to_all(array, axis):
    copies = jnp.broadcast_to(array, (lax.axis_size(axis), *array.shape))
    return lax.all_to_all(copies, axis, split_axis=0, concat_axis=0, tiled=True)


def normalize(tokens, gain):
    values = tokens.astype(F32)
    factor = lax.rsqrt(jnp.mean(values * values, axis=-1, keepdims=True) + norm_eps)
    return (values * factor * gain).astype(BF)


def dot(a, b, ca, cb):
    return lax.dot_general(a, b, (((ca,), (cb,)), ((), ())), preferred_element_type=F32)


def assemble(at, pieces, wholes, sems):
    zb, y = at[0], at[1]
    near, a1, a3, far, z1, z3 = pieces
    todo = []
    for yy in range(4):
        todo.append((near.at[yy], 0, yy))
        todo.append((far.at[yy], 2, yy))
    for r, mine, other in ((1, a1, z1), (3, a3, z3)):
        todo.append((mine, r, y))
        for dy in range(1, 4):
            todo.append((other.at[dy - 1], r, (y + dy) % 4))
    for m, whole in enumerate(wholes):
        for piece, r, yy in todo:
            pltpu.make_async_copy(
                piece.at[:, pl.ds(m * 32, 32), :], whole.at[:, (zb + r) % 4, yy], sems.at[m]
            ).start()


def columns(at, bt, gain, b0, b1, b2, b3, split):
    y = at[1]
    normed = normalize(bt[...], gain[...])
    tiles = [normed[:, z * 128 : (z + 1) * 128].astype(F32) for z in range(16)]
    spot = lax.broadcasted_iota(jnp.int32, (128, 128), 1) // 32
    for yy in range(4):
        for q in range(4):
            tile = tiles[4 * q]
            for j in range(4):
                moved = tiles[4 * q + j]
                if j != yy:
                    moved = pltpu.roll(moved, (j - yy) % 4 * 32, 1)
                tile = jnp.where(spot == j, moved, tile)
            split[yy, :, q * 128 : (q + 1) * 128] = tile.astype(BF)
    for k, out in enumerate((b0, b1, b2, b3)):
        out[...] = split[(y + k) % 4]


def tokens(at, bt, ft, og, gain, out):
    out[0] = normalize(bt[...], gain[...])
    out[1] = og[...]
    out[2] = normalize(ft[...], gain[...])


def products(at, tok, *refs):
    pieces, (gds, keep, give, wg, wu, wd, own, parts, sems, outs) = (
        refs[:6],
        refs[6:],
    )
    assemble(at, pieces, (wg, wu, wd), sems)
    ready = [False] * 3
    stores = []

    def weight(m):
        whole = (wg, wu, wd)[m]
        if not ready[m]:
            pltpu.make_async_copy(whole, whole, sems.at[m]).wait()
            ready[m] = True
        return whole[...].reshape(2048, 352)

    def store(source, target):
        copy = pltpu.make_async_copy(source, target, outs.at[len(stores)])
        copy.start()
        stores.append(copy)

    def store_parts(columns):
        for half, out in ((at[2], keep), (1 - at[2], give)):
            rows = pl.ds(pl.multiple_of(half * 64, 64), 64)
            store(parts.at[rows, columns], out.at[:, columns])

    gate = dot(tok[0], weight(0), 1, 0)
    up = dot(tok[0], weight(1), 1, 0)
    hid = 0.5 * dot(tok[1], weight(2), 1, 0)
    s = jax.nn.sigmoid(gate)
    gd = (hid * up * s * (1.0 + gate * (1.0 - s))).astype(BF)
    ud = (hid * gate * s).astype(BF)
    own[...] = gd.reshape(4, 32, 352)
    for k in range(4):
        store(own, gds.at[k])
    parts[:, 2048:4096] = (dot(gd, weight(0), 1, 1) + dot(ud, weight(1), 1, 1)).astype(BF)
    store_parts(pl.ds(2048, 2048))
    gate = dot(tok[2], weight(0), 1, 0)
    up = dot(tok[2], weight(1), 1, 0)
    hidden = (gate * jax.nn.sigmoid(gate) * up).astype(BF)
    parts[:, 0:2048] = dot(hidden, weight(2), 1, 1).astype(BF)
    store_parts(pl.ds(0, 2048))
    for copy in stores:
        copy.wait()


def merge(at, b0, b1, b2, b3, out):
    for k, piece in enumerate((b0, b1, b2, b3)):
        out[(at[1] + 4 - k) % 4] = piece[...]


def outer(at, cols, gds, grads):
    total = dot(cols[0], gds[0].reshape(128, 352), 0, 0)
    for k in range(1, 4):
        total = total + dot(cols[k], gds[k].reshape(128, 352), 0, 0)
    total = total.astype(BF)
    for z in range(16):
        grads[z] = total[z * 32 : (z + 1) * 32, :]


def pair(at, keep, other, *outs):
    for k, out in enumerate(outs):
        rows = pl.ds(pl.multiple_of((at[3] + k) % 4 * 16, 16), 16)
        out[...] = (keep[rows, :].astype(F32) + other[rows, :].astype(F32)).astype(BF)


def finish(at, p0, p1, p2, p3, bt, gain, out):
    rows = pl.ds(pl.multiple_of((at[2] * 4 + at[3]) * 16, 16), 16)
    total = p0[...].astype(F32) + p1[...].astype(F32) + p2[...].astype(F32) + p3[...].astype(F32)
    out[:, 0:2048] = (0.5 * total[:, 0:2048]).astype(BF)
    values = bt[rows, :].astype(F32)
    factor = lax.rsqrt(jnp.mean(values * values, axis=-1, keepdims=True) + norm_eps)
    scaled = total[:, 2048:4096] * gain[...]
    cubed = factor * factor * factor
    mean = jnp.mean(scaled * values, axis=-1, keepdims=True)
    out[:, 2048:4096] = (factor * scaled - values * cubed * mean).astype(BF)


VM = pl.BlockSpec(memory_space=pltpu.VMEM)
SM = pl.BlockSpec(memory_space=pltpu.SMEM)
ANY = pl.BlockSpec(memory_space=pl.ANY)
DMA = pltpu.SemaphoreType.DMA


def call(body, outs, scratch, *args, ins=None, to=None):
    shape = (lambda o: pltpu.HBM(o, BF)) if to else (lambda o: jax.ShapeDtypeStruct(o, BF))
    return pl.pallas_call(
        body,
        out_shape=tuple(shape(o) for o in outs),
        in_specs=[SM] + (ins or [VM] * (len(args) - 1)),
        out_specs=(to or VM,) * len(outs),
        scratch_shapes=[pltpu.VMEM(o, BF) if isinstance(o, tuple) else o for o in scratch],
        compiler_params=pltpu.CompilerParams(vmem_limit_bytes=LIMIT),
    )(*args)


LIMIT = 24 * 1024 * 1024
W = (4, 4, 4, 32, 352)
TOK = (128, 2048)
COL = (128, 512)


def exchange(array, axis):
    return lax.all_to_all(array, axis, split_axis=0, concat_axis=0, tiled=True)


def shards(ft, bt, og, gain, gw, uw, dw, gsum):
    spots = [lax.axis_index(n) for n in ("zb", "y", "c", "x")]
    y, c = spots[1], spots[2]
    at = jnp.stack(spots).astype(jnp.int32)
    gain = gain.reshape(1, 2048)
    own = jnp.concatenate([gw, uw, dw], axis=0)
    a = copies_to_all(own, "za")
    near = copies_to_all(a, "y")
    a1 = shift(a, Z, -1)
    a3 = shift(a, Z, 1)
    a2 = lax.ppermute(a, Z, [(k, (k + (2 if k % 2 else -2)) % 16) for k in range(16)])
    others = lax.dynamic_slice_in_dim(jnp.concatenate([near, near]), y + 1, 3)
    z1 = shift(others, Z, -1)
    z3 = shift(others, Z, 1)
    far = copies_to_all(a2, "y")
    pieces = (near, a1, a3, far, z1, z3)
    b0, b1, b2, b3 = call(columns, (COL,) * 4, ((4, *COL),), at, bt, gain)
    (tok,) = call(tokens, ((3, *TOK),), (), at, bt, ft, og, gain)
    b1 = shift(b1, "y", 1)
    b2 = shift(b2, "y", 2)
    b3 = shift(b3, "y", 3)
    (cols,) = call(merge, ((4, *COL),), (), at, b0, b1, b2, b3)
    gds, keep, give = call(
        products,
        ((4, 4, 32, 352), (64, 4096), (64, 4096)),
        (W, W, W, (4, 32, 352), (128, 4096), DMA((3,)), DMA((8,))),
        at, tok, *pieces,
        ins=[VM] + [ANY] * 6,
        to=ANY,
    )
    gds = exchange(gds, "y")
    (grads,) = call(outer, ((16, 32, 352),), (), at, cols, gds)
    gz = exchange(grads, Z)
    other = shift(give, "c", 1)
    p0, p1, p2, p3 = call(pair, ((16, 4096),) * 4, (), at, keep, other)
    p1 = shift(p1, "x", 1)
    p2 = shift(p2, "x", 2)
    p3 = shift(p3, "x", -1)
    (done,) = call(finish, ((16, 4096),), (), at, p0, p1, p2, p3, bt, gain)
    half = lax.all_gather(done, "x", axis=0, tiled=True)
    other = shift(half, "c", 1)
    first = jnp.where(c == 0, half, other)
    second = jnp.where(c == 0, other, half)
    whole = jnp.concatenate([first, second], axis=0)
    grad = gsum + gz.astype(F32).sum(axis=0)
    return whole[:, :2048], whole[:, 2048:], grad


def solution(mesh):
    split = Mesh(mesh.devices.reshape(4, 4, 4, 4, 2), ("za", "zb", "y", "x", "c"))
    tok = P(FS, None)
    w = P(FS, TP)
    return jax.shard_map(
        shards,
        mesh=split,
        in_specs=(tok, tok, tok, P(), w, w, w, w),
        out_specs=(tok, tok, w),
        check_vma=False,
    )
```

```python
import jax
import jax.numpy as jnp
from jax import lax
from jax.experimental import pallas as pl
from jax.experimental.pallas import tpu as pltpu
from jax.sharding import Mesh
from jax.sharding import PartitionSpec as P

Z = ("za", "zb")
FS = ("za", "zb", "y")
TP = ("x", "c")
norm_eps = 0.25
F32 = jnp.float32
BF = jnp.bfloat16


def shift(array, axis, by):
    n = lax.axis_size(axis)
    return lax.ppermute(array, axis, [(k, (k + by) % n) for k in range(n)])


def copies_to_all(array, axis):
    copies = jnp.broadcast_to(array, (lax.axis_size(axis), *array.shape))
    return lax.all_to_all(copies, axis, split_axis=0, concat_axis=0, tiled=True)


def normalize(tokens, gain):
    values = tokens.astype(F32)
    factor = lax.rsqrt(jnp.mean(values * values, axis=-1, keepdims=True) + norm_eps)
    return (values * factor * gain).astype(BF)


def dot(a, b, ca, cb):
    return lax.dot_general(a, b, (((ca,), (cb,)), ((), ())), preferred_element_type=F32)


def assemble(at, pieces, wholes, sems):
    zb, y = at[0], at[1]
    near, a1, a3, far, z1, z3 = pieces
    todo = []
    for yy in range(4):
        todo.append((near.at[yy], 0, yy))
        todo.append((far.at[yy], 2, yy))
    for r, mine, other in ((1, a1, z1), (3, a3, z3)):
        todo.append((mine, r, y))
        for dy in range(1, 4):
            todo.append((other.at[dy - 1], r, (y + dy) % 4))
    for m, whole in enumerate(wholes):
        for piece, r, yy in todo:
            pltpu.make_async_copy(
                piece.at[:, pl.ds(m * 32, 32), :], whole.at[:, (zb + r) % 4, yy], sems.at[m]
            ).start()


def move(pairs, sems):
    copies = [pltpu.make_async_copy(a, b, sems.at[k]) for k, (a, b) in enumerate(pairs)]
    for copy in copies:
        copy.start()
    for copy in copies:
        copy.wait()


def spread(at, piece, out, sems):
    move([(piece, out.at[k]) for k in range(4)], sems)


def turn(at, near, out, sems):
    move([(near.at[(at[1] + k) % 4], out.at[k - 1]) for k in range(1, 4)], sems)


def columns(at, bt, gain, b0, b1, b2, b3, split):
    y = at[1]
    normed = normalize(bt[...], gain[...])
    tiles = [normed[:, z * 128 : (z + 1) * 128].astype(F32) for z in range(16)]
    spot = lax.broadcasted_iota(jnp.int32, (128, 128), 1) // 32
    for yy in range(4):
        for q in range(4):
            tile = tiles[4 * q]
            for j in range(4):
                moved = tiles[4 * q + j]
                if j != yy:
                    moved = pltpu.roll(moved, (j - yy) % 4 * 32, 1)
                tile = jnp.where(spot == j, moved, tile)
            split[yy, :, q * 128 : (q + 1) * 128] = tile.astype(BF)
    for k, out in enumerate((b0, b1, b2, b3)):
        out[...] = split[(y + k) % 4]


def tokens(at, bt, ft, og, gain, out):
    out[0] = normalize(bt[...], gain[...])
    out[1] = og[...]
    out[2] = normalize(ft[...], gain[...])


def products(at, tok, *refs):
    pieces, (gds, keep, give, wg, wu, wd, own, parts, sems, outs) = (
        refs[:6],
        refs[6:],
    )
    assemble(at, pieces, (wg, wu, wd), sems)
    ready = [False] * 3
    stores = []

    def weight(m):
        whole = (wg, wu, wd)[m]
        if not ready[m]:
            pltpu.make_async_copy(whole, whole, sems.at[m]).wait()
            ready[m] = True
        return whole[...].reshape(2048, 352)

    def store(source, target):
        copy = pltpu.make_async_copy(source, target, outs.at[len(stores)])
        copy.start()
        stores.append(copy)

    def store_parts(columns):
        for half, out in ((at[2], keep), (1 - at[2], give)):
            rows = pl.ds(pl.multiple_of(half * 64, 64), 64)
            store(parts.at[rows, columns], out.at[:, columns])

    gate = dot(tok[0], weight(0), 1, 0)
    fwd_gate = dot(tok[2], weight(0), 1, 0)
    up = dot(tok[0], weight(1), 1, 0)
    fwd_up = dot(tok[2], weight(1), 1, 0)
    s = jax.nn.sigmoid(gate)
    hidden = (fwd_gate * jax.nn.sigmoid(fwd_gate) * fwd_up).astype(BF)
    hid = 0.5 * dot(tok[1], weight(2), 1, 0)
    gd = (hid * up * s * (1.0 + gate * (1.0 - s))).astype(BF)
    ud = (hid * gate * s).astype(BF)
    own[...] = gd.reshape(4, 32, 352)
    for k in range(4):
        store(own, gds.at[k])
    parts[:, 2048:4096] = (dot(gd, weight(0), 1, 1) + dot(ud, weight(1), 1, 1)).astype(BF)
    store_parts(pl.ds(2048, 2048))
    parts[:, 0:2048] = dot(hidden, weight(2), 1, 1).astype(BF)
    store_parts(pl.ds(0, 2048))
    for copy in stores:
        copy.wait()


def merge(at, b0, b1, b2, b3, out):
    for k, piece in enumerate((b0, b1, b2, b3)):
        out[(at[1] + 4 - k) % 4] = piece[...]


def outer(at, cols, gds, grads):
    total = dot(cols[0], gds[0].reshape(128, 352), 0, 0)
    for k in range(1, 4):
        total = total + dot(cols[k], gds[k].reshape(128, 352), 0, 0)
    total = total.astype(BF)
    for z in range(16):
        grads[z] = total[z * 32 : (z + 1) * 32, :]


def pair(at, keep, other, *outs):
    for k, out in enumerate(outs):
        rows = pl.ds(pl.multiple_of((at[3] + k) % 4 * 16, 16), 16)
        out[...] = (keep[rows, :].astype(F32) + other[rows, :].astype(F32)).astype(BF)


def finish(at, p0, p1, p2, p3, bt, gain, out):
    rows = pl.ds(pl.multiple_of((at[2] * 4 + at[3]) * 16, 16), 16)
    total = p0[...].astype(F32) + p1[...].astype(F32) + p2[...].astype(F32) + p3[...].astype(F32)
    out[:, 0:2048] = (0.5 * total[:, 0:2048]).astype(BF)
    values = bt[rows, :].astype(F32)
    factor = lax.rsqrt(jnp.mean(values * values, axis=-1, keepdims=True) + norm_eps)
    scaled = total[:, 2048:4096] * gain[...]
    cubed = factor * factor * factor
    mean = jnp.mean(scaled * values, axis=-1, keepdims=True)
    out[:, 2048:4096] = (factor * scaled - values * cubed * mean).astype(BF)


VM = pl.BlockSpec(memory_space=pltpu.VMEM)
SM = pl.BlockSpec(memory_space=pltpu.SMEM)
ANY = pl.BlockSpec(memory_space=pl.ANY)
DMA = pltpu.SemaphoreType.DMA


def call(body, outs, scratch, *args, ins=None, to=None):
    shape = (lambda o: pltpu.HBM(o, BF)) if to else (lambda o: jax.ShapeDtypeStruct(o, BF))
    return pl.pallas_call(
        body,
        out_shape=tuple(shape(o) for o in outs),
        in_specs=[SM] + (ins or [VM] * (len(args) - 1)),
        out_specs=(to or VM,) * len(outs),
        scratch_shapes=[pltpu.VMEM(o, BF) if isinstance(o, tuple) else o for o in scratch],
        compiler_params=pltpu.CompilerParams(vmem_limit_bytes=LIMIT),
    )(*args)


LIMIT = 24 * 1024 * 1024
W = (4, 4, 4, 32, 352)
SETS = (4, 4, 96, 352)
TOK = (128, 2048)
COL = (128, 512)


def exchange(array, axis):
    return lax.all_to_all(array, axis, split_axis=0, concat_axis=0, tiled=True)


def shards(ft, bt, og, gain, gw, uw, dw, gsum):
    spots = [lax.axis_index(n) for n in ("zb", "y", "c", "x")]
    c = spots[2]
    at = jnp.stack(spots).astype(jnp.int32)
    gain = gain.reshape(1, 2048)
    own = jnp.concatenate([gw, uw, dw], axis=0)
    a = copies_to_all(own, "za")
    (copies,) = call(spread, (SETS,), (DMA((4,)),), at, a, ins=[ANY], to=ANY)
    near = exchange(copies, "y")
    a1 = shift(a, Z, -1)
    a3 = shift(a, Z, 1)
    a2 = lax.ppermute(a, Z, [(k, (k + (2 if k % 2 else -2)) % 16) for k in range(16)])
    (others,) = call(turn, ((3, 4, 96, 352),), (DMA((3,)),), at, near, ins=[ANY], to=ANY)
    z1 = shift(others, Z, -1)
    z3 = shift(others, Z, 1)
    (copies,) = call(spread, (SETS,), (DMA((4,)),), at, a2, ins=[ANY], to=ANY)
    far = exchange(copies, "y")
    pieces = (near, a1, a3, far, z1, z3)
    b0, b1, b2, b3 = call(columns, (COL,) * 4, ((4, *COL),), at, bt, gain)
    (tok,) = call(tokens, ((3, *TOK),), (), at, bt, ft, og, gain)
    b1 = shift(b1, "y", 1)
    b2 = shift(b2, "y", 2)
    b3 = shift(b3, "y", 3)
    (cols,) = call(merge, ((4, *COL),), (), at, b0, b1, b2, b3)
    gds, keep, give = call(
        products,
        ((4, 4, 32, 352), (64, 4096), (64, 4096)),
        (W, W, W, (4, 32, 352), (128, 4096), DMA((3,)), DMA((8,))),
        at, tok, *pieces,
        ins=[VM] + [ANY] * 6,
        to=ANY,
    )
    gds = exchange(gds, "y")
    (grads,) = call(outer, ((16, 32, 352),), (), at, cols, gds)
    gz = exchange(grads, Z)
    other = shift(give, "c", 1)
    p0, p1, p2, p3 = call(pair, ((16, 4096),) * 4, (), at, keep, other)
    p1 = shift(p1, "x", 1)
    p2 = shift(p2, "x", 2)
    p3 = shift(p3, "x", -1)
    (done,) = call(finish, ((16, 4096),), (), at, p0, p1, p2, p3, bt, gain)
    half = lax.all_gather(done, "x", axis=0, tiled=True)
    other = shift(half, "c", 1)
    first = jnp.where(c == 0, half, other)
    second = jnp.where(c == 0, other, half)
    whole = jnp.concatenate([first, second], axis=0)
    grad = gsum + gz.astype(F32).sum(axis=0)
    return whole[:, :2048], whole[:, 2048:], grad


def solution(mesh):
    split = Mesh(mesh.devices.reshape(4, 4, 4, 4, 2), ("za", "zb", "y", "x", "c"))
    tok = P(FS, None)
    w = P(FS, TP)
    return jax.shard_map(
        shards,
        mesh=split,
        in_specs=(tok, tok, tok, P(), w, w, w, w),
        out_specs=(tok, tok, w),
        check_vma=False,
    )
```

```python
import jax
import jax.numpy as jnp
from jax import lax
from jax.experimental import pallas as pl
from jax.experimental.pallas import tpu as pltpu
from jax.sharding import Mesh
from jax.sharding import PartitionSpec as P

Z = ("za", "zb")
FS = ("za", "zb", "y")
TP = ("x", "c")
norm_eps = 0.25
F32 = jnp.float32
BF = jnp.bfloat16


def shift(array, axis, by):
    n = lax.axis_size(axis)
    return lax.ppermute(array, axis, [(k, (k + by) % n) for k in range(n)])


def copies_to_all(array, axis):
    copies = jnp.broadcast_to(array, (lax.axis_size(axis), *array.shape))
    return lax.all_to_all(copies, axis, split_axis=0, concat_axis=0, tiled=True)


def normalize(tokens, gain):
    values = tokens.astype(F32)
    factor = lax.rsqrt(jnp.mean(values * values, axis=-1, keepdims=True) + norm_eps)
    return (values * factor * gain).astype(BF)


def dot(a, b, ca, cb):
    return lax.dot_general(a, b, (((ca,), (cb,)), ((), ())), preferred_element_type=F32)


def assemble(at, pieces, whole, sem):
    zb, y = at[0], at[1]
    near, a1, a3, far, z1, z3 = pieces
    todo = []
    for yy in range(4):
        todo.append((near.at[yy], 0, yy))
        todo.append((far.at[yy], 2, yy))
    for r, mine, other in ((1, a1, z1), (3, a3, z3)):
        todo.append((mine, r, y))
        for dy in range(1, 4):
            todo.append((other.at[dy - 1], r, (y + dy) % 4))
    for piece, r, yy in todo:
        pltpu.make_async_copy(piece, whole.at[:, (zb + r) % 4, yy], sem).start()
    pltpu.make_async_copy(whole, whole, sem).wait()


def move(pairs, sems):
    copies = [pltpu.make_async_copy(a, b, sems.at[k]) for k, (a, b) in enumerate(pairs)]
    for copy in copies:
        copy.start()
    for copy in copies:
        copy.wait()


def spread(at, piece, out, sems):
    move([(piece, out.at[k]) for k in range(4)], sems)


def turn(at, near, out, sems):
    move([(near.at[(at[1] + k) % 4], out.at[k - 1]) for k in range(1, 4)], sems)


def columns(at, bt, gain, b0, b1, b2, b3, split):
    y = at[1]
    normed = normalize(bt[...], gain[...])
    tiles = [normed[:, z * 128 : (z + 1) * 128].astype(F32) for z in range(16)]
    spot = lax.broadcasted_iota(jnp.int32, (128, 128), 1) // 32
    for yy in range(4):
        for q in range(4):
            tile = tiles[4 * q]
            for j in range(4):
                moved = tiles[4 * q + j]
                if j != yy:
                    moved = pltpu.roll(moved, (j - yy) % 4 * 32, 1)
                tile = jnp.where(spot == j, moved, tile)
            split[yy, :, q * 128 : (q + 1) * 128] = tile.astype(BF)
    for k, out in enumerate((b0, b1, b2, b3)):
        out[...] = split[(y + k) % 4]


def tokens(at, bt, ft, og, gain, out):
    out[0] = normalize(bt[...], gain[...])
    out[1] = og[...]
    out[2] = normalize(ft[...], gain[...])


def products(at, tok, *refs):
    pieces, (gds, keep, give, whole, own, parts, sem, outs) = (
        refs[:6],
        refs[6:],
    )
    assemble(at, pieces, whole, sem)
    stores = []

    def weight(m):
        return whole[:, :, :, m * 32 : (m + 1) * 32, :].reshape(2048, 352)

    def store(source, target):
        copy = pltpu.make_async_copy(source, target, outs.at[len(stores)])
        copy.start()
        stores.append(copy)

    def store_parts(columns):
        for half, out in ((at[2], keep), (1 - at[2], give)):
            rows = pl.ds(pl.multiple_of(half * 64, 64), 64)
            store(parts.at[rows, columns], out.at[:, columns])

    gate = dot(tok[0], weight(0), 1, 0)
    fwd_gate = dot(tok[2], weight(0), 1, 0)
    up = dot(tok[0], weight(1), 1, 0)
    fwd_up = dot(tok[2], weight(1), 1, 0)
    s = jax.nn.sigmoid(gate)
    hidden = (fwd_gate * jax.nn.sigmoid(fwd_gate) * fwd_up).astype(BF)
    hid = 0.5 * dot(tok[1], weight(2), 1, 0)
    gd = (hid * up * s * (1.0 + gate * (1.0 - s))).astype(BF)
    ud = (hid * gate * s).astype(BF)
    own[...] = gd.reshape(4, 32, 352)
    for k in range(4):
        store(own, gds.at[k])
    parts[:, 2048:4096] = (dot(gd, weight(0), 1, 1) + dot(ud, weight(1), 1, 1)).astype(BF)
    store_parts(pl.ds(2048, 2048))
    parts[:, 0:2048] = dot(hidden, weight(2), 1, 1).astype(BF)
    store_parts(pl.ds(0, 2048))
    for copy in stores:
        copy.wait()


def merge(at, b0, b1, b2, b3, out):
    for k, piece in enumerate((b0, b1, b2, b3)):
        spot = pl.multiple_of((at[1] + 4 - k) % 4 * 128, 128)
        out[:, pl.ds(spot, 128)] = piece[...].astype(F32).T.astype(BF)


def outer(at, cols, gds, grads):
    total = dot(cols[...], gds[...].reshape(512, 352), 1, 0).astype(BF)
    for z in range(16):
        grads[z] = total[z * 32 : (z + 1) * 32, :]


def pair(at, keep, other, *outs):
    for k, out in enumerate(outs):
        rows = pl.ds(pl.multiple_of((at[3] + k) % 4 * 16, 16), 16)
        out[...] = (keep[rows, :].astype(F32) + other[rows, :].astype(F32)).astype(BF)


def finish(at, p0, p1, p2, p3, bt, gain, out):
    rows = pl.ds(pl.multiple_of((at[2] * 4 + at[3]) * 16, 16), 16)
    total = p0[...].astype(F32) + p1[...].astype(F32) + p2[...].astype(F32) + p3[...].astype(F32)
    out[:, 0:2048] = (0.5 * total[:, 0:2048]).astype(BF)
    values = bt[rows, :].astype(F32)
    factor = lax.rsqrt(jnp.mean(values * values, axis=-1, keepdims=True) + norm_eps)
    scaled = total[:, 2048:4096] * gain[...]
    cubed = factor * factor * factor
    mean = jnp.mean(scaled * values, axis=-1, keepdims=True)
    out[:, 2048:4096] = (factor * scaled - values * cubed * mean).astype(BF)


VM = pl.BlockSpec(memory_space=pltpu.VMEM)
SM = pl.BlockSpec(memory_space=pltpu.SMEM)
ANY = pl.BlockSpec(memory_space=pl.ANY)
DMA = pltpu.SemaphoreType.DMA


def call(body, outs, scratch, *args, ins=None, to=None):
    shape = (lambda o: pltpu.HBM(o, BF)) if to else (lambda o: jax.ShapeDtypeStruct(o, BF))
    return pl.pallas_call(
        body,
        out_shape=tuple(shape(o) for o in outs),
        in_specs=[SM] + (ins or [VM] * (len(args) - 1)),
        out_specs=(to or VM,) * len(outs),
        scratch_shapes=[pltpu.VMEM(o, BF) if isinstance(o, tuple) else o for o in scratch],
        compiler_params=pltpu.CompilerParams(vmem_limit_bytes=LIMIT),
    )(*args)


LIMIT = 24 * 1024 * 1024
W = (4, 4, 4, 96, 352)
SETS = (4, 4, 96, 352)
TOK = (128, 2048)
COL = (128, 512)


def exchange(array, axis):
    return lax.all_to_all(array, axis, split_axis=0, concat_axis=0, tiled=True)


def shards(ft, bt, og, gain, gw, uw, dw, gsum):
    spots = [lax.axis_index(n) for n in ("zb", "y", "c", "x")]
    c = spots[2]
    at = jnp.stack(spots).astype(jnp.int32)
    gain = gain.reshape(1, 2048)
    own = jnp.concatenate([gw, uw, dw], axis=0)
    a = copies_to_all(own, "za")
    (copies,) = call(spread, (SETS,), (DMA((4,)),), at, a, ins=[ANY], to=ANY)
    near = exchange(copies, "y")
    a1 = shift(a, Z, -1)
    a3 = shift(a, Z, 1)
    a2 = lax.ppermute(a, Z, [(k, (k + (2 if k % 2 else -2)) % 16) for k in range(16)])
    (others,) = call(turn, ((3, 4, 96, 352),), (DMA((3,)),), at, near, ins=[ANY], to=ANY)
    z1 = shift(others, Z, -1)
    z3 = shift(others, Z, 1)
    (copies,) = call(spread, (SETS,), (DMA((4,)),), at, a2, ins=[ANY], to=ANY)
    far = exchange(copies, "y")
    pieces = (near, a1, a3, far, z1, z3)
    b0, b1, b2, b3 = call(columns, (COL,) * 4, ((4, *COL),), at, bt, gain)
    (tok,) = call(tokens, ((3, *TOK),), (), at, bt, ft, og, gain)
    b1 = shift(b1, "y", 1)
    b2 = shift(b2, "y", 2)
    b3 = shift(b3, "y", 3)
    (cols,) = call(merge, ((512, 512),), (), at, b0, b1, b2, b3)
    gds, keep, give = call(
        products,
        ((4, 4, 32, 352), (64, 4096), (64, 4096)),
        (W, (4, 32, 352), (128, 4096), DMA, DMA((8,))),
        at, tok, *pieces,
        ins=[VM] + [ANY] * 6,
        to=ANY,
    )
    gds = exchange(gds, "y")
    (grads,) = call(outer, ((16, 32, 352),), (), at, cols, gds)
    gz = exchange(grads, Z)
    other = shift(give, "c", 1)
    p0, p1, p2, p3 = call(pair, ((16, 4096),) * 4, (), at, keep, other)
    p1 = shift(p1, "x", 1)
    p2 = shift(p2, "x", 2)
    p3 = shift(p3, "x", -1)
    (done,) = call(finish, ((16, 4096),), (), at, p0, p1, p2, p3, bt, gain)
    half = lax.all_gather(done, "x", axis=0, tiled=True)
    other = shift(half, "c", 1)
    first = jnp.where(c == 0, half, other)
    second = jnp.where(c == 0, other, half)
    whole = jnp.concatenate([first, second], axis=0)
    grad = gsum + gz.astype(F32).sum(axis=0)
    return whole[:, :2048], whole[:, 2048:], grad


def solution(mesh):
    split = Mesh(mesh.devices.reshape(4, 4, 4, 4, 2), ("za", "zb", "y", "x", "c"))
    tok = P(FS, None)
    w = P(FS, TP)
    return jax.shard_map(
        shards,
        mesh=split,
        in_specs=(tok, tok, tok, P(), w, w, w, w),
        out_specs=(tok, tok, w),
        check_vma=False,
    )
```

```python
import jax
import jax.numpy as jnp
from jax import lax
from jax.experimental import pallas as pl
from jax.experimental.pallas import tpu as pltpu
from jax.sharding import Mesh
from jax.sharding import PartitionSpec as P

Z = ("za", "zb")
FS = ("za", "zb", "y")
TP = ("x", "c")
norm_eps = 0.25
F32 = jnp.float32
BF = jnp.bfloat16


def shift(array, axis, by):
    n = lax.axis_size(axis)
    return lax.ppermute(array, axis, [(k, (k + by) % n) for k in range(n)])


def copies_to_all(array, axis):
    copies = jnp.broadcast_to(array, (lax.axis_size(axis), *array.shape))
    return lax.all_to_all(copies, axis, split_axis=0, concat_axis=0, tiled=True)


def normalize(tokens, gain):
    values = tokens.astype(F32)
    factor = lax.rsqrt(jnp.mean(values * values, axis=-1, keepdims=True) + norm_eps)
    return (values * factor * gain).astype(BF)


def dot(a, b, ca, cb):
    return lax.dot_general(a, b, (((ca,), (cb,)), ((), ())), preferred_element_type=F32)


def assemble(at, pieces, wholes, sems):
    zb, y = at[0], at[1]
    near, a1, a3, far, z1, z3 = pieces
    todo = []
    for yy in range(4):
        todo.append((near.at[yy], 0, yy))
        todo.append((far.at[yy], 2, yy))
    for r, mine, other in ((1, a1, z1), (3, a3, z3)):
        todo.append((mine, r, y))
        for dy in range(1, 4):
            todo.append((other.at[dy - 1], r, (y + dy) % 4))
    for m, whole in enumerate(wholes):
        for piece, r, yy in todo:
            pltpu.make_async_copy(
                piece.at[:, pl.ds(m * 32, 32), :], whole.at[:, (zb + r) % 4, yy], sems.at[m]
            ).start()


def move(pairs, sems):
    copies = [pltpu.make_async_copy(a, b, sems.at[k]) for k, (a, b) in enumerate(pairs)]
    for copy in copies:
        copy.start()
    for copy in copies:
        copy.wait()


def spread(at, piece, out, sems):
    move([(piece, out.at[k]) for k in range(4)], sems)


def turn(at, near, out, sems):
    move([(near.at[(at[1] + k) % 4], out.at[k - 1]) for k in range(1, 4)], sems)


def place(at, half, other, fwd, back, sems):
    pairs = []
    for part, c in ((half, at[2]), (other, 1 - at[2])):
        rows = pl.ds(pl.multiple_of(c * 64, 64), 64)
        pairs.append((part.at[:, pl.ds(0, 2048)], fwd.at[rows, :]))
        pairs.append((part.at[:, pl.ds(2048, 2048)], back.at[rows, :]))
    move(pairs, sems)


def columns(at, bt, gain, b0, b1, b2, b3, split):
    y = at[1]
    normed = normalize(bt[...], gain[...])
    tiles = [normed[:, z * 128 : (z + 1) * 128].astype(F32) for z in range(16)]
    spot = lax.broadcasted_iota(jnp.int32, (128, 128), 1) // 32
    for yy in range(4):
        for q in range(4):
            tile = tiles[4 * q]
            for j in range(4):
                moved = tiles[4 * q + j]
                if j != yy:
                    moved = pltpu.roll(moved, (j - yy) % 4 * 32, 1)
                tile = jnp.where(spot == j, moved, tile)
            split[yy, :, q * 128 : (q + 1) * 128] = tile.astype(BF)
    for k, out in enumerate((b0, b1, b2, b3)):
        out[...] = split[(y + k) % 4]


def tokens(at, bt, ft, og, gain, out):
    out[0] = normalize(bt[...], gain[...])
    out[1] = og[...]
    out[2] = normalize(ft[...], gain[...])


def products(at, tok, *refs):
    pieces, (gds, keep, give, wg, wu, wd, own, parts, sems, outs) = (
        refs[:6],
        refs[6:],
    )
    assemble(at, pieces, (wg, wu, wd), sems)
    ready = [False] * 3
    stores = []

    def weight(m):
        whole = (wg, wu, wd)[m]
        if not ready[m]:
            pltpu.make_async_copy(whole, whole, sems.at[m]).wait()
            ready[m] = True
        return whole[...].reshape(2048, 352)

    def store(source, target):
        copy = pltpu.make_async_copy(source, target, outs.at[len(stores)])
        copy.start()
        stores.append(copy)

    def store_parts(columns):
        for half, out in ((at[2], keep), (1 - at[2], give)):
            rows = pl.ds(pl.multiple_of(half * 64, 64), 64)
            store(parts.at[rows, columns], out.at[:, columns])

    gate = dot(tok[0], weight(0), 1, 0)
    fwd_gate = dot(tok[2], weight(0), 1, 0)
    up = dot(tok[0], weight(1), 1, 0)
    fwd_up = dot(tok[2], weight(1), 1, 0)
    s = jax.nn.sigmoid(gate)
    hidden = (fwd_gate * jax.nn.sigmoid(fwd_gate) * fwd_up).astype(BF)
    hid = 0.5 * dot(tok[1], weight(2), 1, 0)
    gd = (hid * up * s * (1.0 + gate * (1.0 - s))).astype(BF)
    ud = (hid * gate * s).astype(BF)
    own[...] = gd.reshape(4, 32, 352)
    for k in range(4):
        store(own, gds.at[k])
    parts[:, 2048:4096] = (dot(gd, weight(0), 1, 1) + dot(ud, weight(1), 1, 1)).astype(BF)
    store_parts(pl.ds(2048, 2048))
    parts[:, 0:2048] = dot(hidden, weight(2), 1, 1).astype(BF)
    store_parts(pl.ds(0, 2048))
    for copy in stores:
        copy.wait()


def merge(at, b0, b1, b2, b3, out):
    for k, piece in enumerate((b0, b1, b2, b3)):
        spot = pl.multiple_of((at[1] + 4 - k) % 4 * 128, 128)
        out[:, pl.ds(spot, 128)] = piece[...].astype(F32).T.astype(BF)


def outer(at, cols, gds, grads):
    total = dot(cols[...], gds[...].reshape(512, 352), 1, 0).astype(BF)
    for z in range(16):
        grads[z] = total[z * 32 : (z + 1) * 32, :]


def pair(at, keep, other, *outs):
    for k, out in enumerate(outs):
        rows = pl.ds(pl.multiple_of((at[3] + k) % 4 * 16, 16), 16)
        out[...] = (keep[rows, :].astype(F32) + other[rows, :].astype(F32)).astype(BF)


def finish(at, p0, p1, p2, p3, bt, gain, out):
    rows = pl.ds(pl.multiple_of((at[2] * 4 + at[3]) * 16, 16), 16)
    total = p0[...].astype(F32) + p1[...].astype(F32) + p2[...].astype(F32) + p3[...].astype(F32)
    out[:, 0:2048] = (0.5 * total[:, 0:2048]).astype(BF)
    values = bt[rows, :].astype(F32)
    factor = lax.rsqrt(jnp.mean(values * values, axis=-1, keepdims=True) + norm_eps)
    scaled = total[:, 2048:4096] * gain[...]
    cubed = factor * factor * factor
    mean = jnp.mean(scaled * values, axis=-1, keepdims=True)
    out[:, 2048:4096] = (factor * scaled - values * cubed * mean).astype(BF)


VM = pl.BlockSpec(memory_space=pltpu.VMEM)
SM = pl.BlockSpec(memory_space=pltpu.SMEM)
ANY = pl.BlockSpec(memory_space=pl.ANY)
DMA = pltpu.SemaphoreType.DMA


def call(body, outs, scratch, *args, ins=None, to=None):
    shape = (lambda o: pltpu.HBM(o, BF)) if to else (lambda o: jax.ShapeDtypeStruct(o, BF))
    return pl.pallas_call(
        body,
        out_shape=tuple(shape(o) for o in outs),
        in_specs=[SM] + (ins or [VM] * (len(args) - 1)),
        out_specs=(to or VM,) * len(outs),
        scratch_shapes=[pltpu.VMEM(o, BF) if isinstance(o, tuple) else o for o in scratch],
        compiler_params=pltpu.CompilerParams(vmem_limit_bytes=LIMIT),
    )(*args)


LIMIT = 24 * 1024 * 1024
W = (4, 4, 4, 32, 352)
SETS = (4, 4, 96, 352)
TOK = (128, 2048)
COL = (128, 512)


def exchange(array, axis):
    return lax.all_to_all(array, axis, split_axis=0, concat_axis=0, tiled=True)


def shards(ft, bt, og, gain, gw, uw, dw, gsum):
    spots = [lax.axis_index(n) for n in ("zb", "y", "c", "x")]
    at = jnp.stack(spots).astype(jnp.int32)
    gain = gain.reshape(1, 2048)
    own = jnp.concatenate([gw, uw, dw], axis=0)
    a = copies_to_all(own, "za")
    (copies,) = call(spread, (SETS,), (DMA((4,)),), at, a, ins=[ANY], to=ANY)
    near = exchange(copies, "y")
    a1 = shift(a, Z, -1)
    a3 = shift(a, Z, 1)
    a2 = lax.ppermute(a, Z, [(k, (k + (2 if k % 2 else -2)) % 16) for k in range(16)])
    (others,) = call(turn, ((3, 4, 96, 352),), (DMA((3,)),), at, near, ins=[ANY], to=ANY)
    z1 = shift(others, Z, -1)
    z3 = shift(others, Z, 1)
    (copies,) = call(spread, (SETS,), (DMA((4,)),), at, a2, ins=[ANY], to=ANY)
    far = exchange(copies, "y")
    pieces = (near, a1, a3, far, z1, z3)
    b0, b1, b2, b3 = call(columns, (COL,) * 4, ((4, *COL),), at, bt, gain)
    (tok,) = call(tokens, ((3, *TOK),), (), at, bt, ft, og, gain)
    b1 = shift(b1, "y", 1)
    b2 = shift(b2, "y", 2)
    b3 = shift(b3, "y", 3)
    (cols,) = call(merge, ((512, 512),), (), at, b0, b1, b2, b3)
    gds, keep, give = call(
        products,
        ((4, 4, 32, 352), (64, 4096), (64, 4096)),
        (W, W, W, (4, 32, 352), (128, 4096), DMA((3,)), DMA((8,))),
        at, tok, *pieces,
        ins=[VM] + [ANY] * 6,
        to=ANY,
    )
    gds = exchange(gds, "y")
    (grads,) = call(outer, ((16, 32, 352),), (), at, cols, gds)
    gz = exchange(grads, Z)
    other = shift(give, "c", 1)
    p0, p1, p2, p3 = call(pair, ((16, 4096),) * 4, (), at, keep, other)
    p1 = shift(p1, "x", 1)
    p2 = shift(p2, "x", 2)
    p3 = shift(p3, "x", -1)
    (done,) = call(finish, ((16, 4096),), (), at, p0, p1, p2, p3, bt, gain)
    half = lax.all_gather(done, "x", axis=0, tiled=True)
    other = shift(half, "c", 1)
    fwd, back = call(place, (TOK, TOK), (DMA((4,)),), at, half, other, ins=[ANY] * 2, to=ANY)
    grad = gsum + gz.astype(F32).sum(axis=0)
    return fwd, back, grad


def solution(mesh):
    split = Mesh(mesh.devices.reshape(4, 4, 4, 4, 2), ("za", "zb", "y", "x", "c"))
    tok = P(FS, None)
    w = P(FS, TP)
    return jax.shard_map(
        shards,
        mesh=split,
        in_specs=(tok, tok, tok, P(), w, w, w, w),
        out_specs=(tok, tok, w),
        check_vma=False,
    )
```

```python
import jax
import jax.numpy as jnp
from jax import lax
from jax.experimental import pallas as pl
from jax.experimental.pallas import tpu as pltpu
from jax.sharding import Mesh
from jax.sharding import PartitionSpec as P

Z = ("za", "zb")
FS = ("za", "zb", "y")
TP = ("x", "c")
norm_eps = 0.25
F32 = jnp.float32
BF = jnp.bfloat16


def shift(array, axis, by):
    n = lax.axis_size(axis)
    return lax.ppermute(array, axis, [(k, (k + by) % n) for k in range(n)])


def copies_to_all(array, axis):
    copies = jnp.broadcast_to(array, (lax.axis_size(axis), *array.shape))
    return lax.all_to_all(copies, axis, split_axis=0, concat_axis=0, tiled=True)


def normalize(tokens, gain):
    values = tokens.astype(F32)
    factor = lax.rsqrt(jnp.mean(values * values, axis=-1, keepdims=True) + norm_eps)
    return (values * factor * gain).astype(BF)


def dot(a, b, ca, cb):
    return lax.dot_general(a, b, (((ca,), (cb,)), ((), ())), preferred_element_type=F32)


def assemble(at, pieces, wholes, sems):
    zb, y = at[0], at[1]
    near, a1, a3, far, z1, z3 = pieces
    todo = []
    for yy in range(4):
        todo.append((near.at[yy], 0, yy))
        todo.append((far.at[yy], 2, yy))
    for r, mine, other in ((1, a1, z1), (3, a3, z3)):
        todo.append((mine, r, y))
        for dy in range(1, 4):
            todo.append((other.at[dy - 1], r, (y + dy) % 4))
    for m, whole in enumerate(wholes):
        for piece, r, yy in todo:
            pltpu.make_async_copy(
                piece.at[:, pl.ds(m * 32, 32), :], whole.at[:, (zb + r) % 4, yy], sems.at[m]
            ).start()


def move(pairs, sems):
    copies = [pltpu.make_async_copy(a, b, sems.at[k]) for k, (a, b) in enumerate(pairs)]
    for copy in copies:
        copy.start()
    for copy in copies:
        copy.wait()


def spread(at, piece, out, sems):
    move([(piece, out.at[k]) for k in range(4)], sems)


def turn(at, near, out, sems):
    move([(near.at[(at[1] + k) % 4], out.at[k - 1]) for k in range(1, 4)], sems)


def columns(at, bt, gain, b0, b1, b2, b3, split):
    y = at[1]
    normed = normalize(bt[...], gain[...])
    tiles = [normed[:, z * 128 : (z + 1) * 128].astype(F32) for z in range(16)]
    spot = lax.broadcasted_iota(jnp.int32, (128, 128), 1) // 32
    for yy in range(4):
        for q in range(4):
            tile = tiles[4 * q]
            for j in range(4):
                moved = tiles[4 * q + j]
                if j != yy:
                    moved = pltpu.roll(moved, (j - yy) % 4 * 32, 1)
                tile = jnp.where(spot == j, moved, tile)
            split[yy, :, q * 128 : (q + 1) * 128] = tile.astype(BF)
    for k, out in enumerate((b0, b1, b2, b3)):
        out[...] = split[(y + k) % 4]


def tokens(at, bt, ft, og, gain, out):
    out[0] = normalize(bt[...], gain[...])
    out[1] = og[...]
    out[2] = normalize(ft[...], gain[...])


def products(at, tok, *refs):
    pieces, (gds, keep, give, wg, wu, wd, own, parts, sems, outs) = (
        refs[:6],
        refs[6:],
    )
    assemble(at, pieces, (wg, wu, wd), sems)
    ready = [False] * 3
    stores = []

    def weight(m):
        whole = (wg, wu, wd)[m]
        if not ready[m]:
            pltpu.make_async_copy(whole, whole, sems.at[m]).wait()
            ready[m] = True
        return whole[...].reshape(2048, 352)

    def store(source, target):
        copy = pltpu.make_async_copy(source, target, outs.at[len(stores)])
        copy.start()
        stores.append(copy)

    def store_parts(columns):
        for half, out in ((at[2], keep), (1 - at[2], give)):
            rows = pl.ds(pl.multiple_of(half * 64, 64), 64)
            store(parts.at[rows, columns], out.at[:, columns])

    gate = dot(tok[0], weight(0), 1, 0)
    fwd_gate = dot(tok[2], weight(0), 1, 0)
    up = dot(tok[0], weight(1), 1, 0)
    fwd_up = dot(tok[2], weight(1), 1, 0)
    s = jax.nn.sigmoid(gate)
    hidden = (fwd_gate * jax.nn.sigmoid(fwd_gate) * fwd_up).astype(BF)
    hid = 0.5 * dot(tok[1], weight(2), 1, 0)
    gd = (hid * up * s * (1.0 + gate * (1.0 - s))).astype(BF)
    ud = (hid * gate * s).astype(BF)
    own[...] = gd.reshape(4, 32, 352)
    for k in range(4):
        store(own, gds.at[k])
    parts[:, 2048:4096] = (dot(gd, weight(0), 1, 1) + dot(ud, weight(1), 1, 1)).astype(BF)
    store_parts(pl.ds(2048, 2048))
    parts[:, 0:2048] = dot(hidden, weight(2), 1, 1).astype(BF)
    store_parts(pl.ds(0, 2048))
    for copy in stores:
        copy.wait()


def merge(at, b0, b1, b2, b3, out):
    for k, piece in enumerate((b0, b1, b2, b3)):
        spot = pl.multiple_of((at[1] + 4 - k) % 4 * 128, 128)
        out[:, pl.ds(spot, 128)] = piece[...].astype(F32).T.astype(BF)


def outer(at, cols, gds, grads):
    total = dot(cols[...], gds[...].reshape(512, 352), 1, 0).astype(BF)
    for z in range(16):
        grads[z] = total[z * 32 : (z + 1) * 32, :]


def pair(at, keep, other, *outs):
    for k, out in enumerate(outs):
        rows = pl.ds(pl.multiple_of((at[3] + k) % 4 * 16, 16), 16)
        out[...] = (keep[rows, :].astype(F32) + other[rows, :].astype(F32)).astype(BF)


def finish(at, p0, p1, p2, p3, bt, gain, out):
    rows = pl.ds(pl.multiple_of((at[2] * 4 + at[3]) * 16, 16), 16)
    total = p0[...].astype(F32) + p1[...].astype(F32) + p2[...].astype(F32) + p3[...].astype(F32)
    out[:, 0:2048] = (0.5 * total[:, 0:2048]).astype(BF)
    values = bt[rows, :].astype(F32)
    factor = lax.rsqrt(jnp.mean(values * values, axis=-1, keepdims=True) + norm_eps)
    scaled = total[:, 2048:4096] * gain[...]
    cubed = factor * factor * factor
    mean = jnp.mean(scaled * values, axis=-1, keepdims=True)
    out[:, 2048:4096] = (factor * scaled - values * cubed * mean).astype(BF)


VM = pl.BlockSpec(memory_space=pltpu.VMEM)
SM = pl.BlockSpec(memory_space=pltpu.SMEM)
ANY = pl.BlockSpec(memory_space=pl.ANY)
DMA = pltpu.SemaphoreType.DMA


def call(body, outs, scratch, *args, ins=None, to=None):
    shape = (lambda o: pltpu.HBM(o, BF)) if to else (lambda o: jax.ShapeDtypeStruct(o, BF))
    return pl.pallas_call(
        body,
        out_shape=tuple(shape(o) for o in outs),
        in_specs=[SM] + (ins or [VM] * (len(args) - 1)),
        out_specs=(to or VM,) * len(outs),
        scratch_shapes=[pltpu.VMEM(o, BF) if isinstance(o, tuple) else o for o in scratch],
        compiler_params=pltpu.CompilerParams(vmem_limit_bytes=LIMIT),
    )(*args)


LIMIT = 24 * 1024 * 1024
W = (4, 4, 4, 32, 352)
SETS = (4, 4, 96, 352)
TOK = (128, 2048)
COL = (128, 512)


def exchange(array, axis):
    return lax.all_to_all(array, axis, split_axis=0, concat_axis=0, tiled=True)


def shards(ft, bt, og, gain, gw, uw, dw, gsum):
    spots = [lax.axis_index(n) for n in ("zb", "y", "c", "x")]
    c = spots[2]
    at = jnp.stack(spots).astype(jnp.int32)
    gain = gain.reshape(1, 2048)
    own = jnp.concatenate([gw, uw, dw], axis=0)
    a = copies_to_all(own, "za")
    (copies,) = call(spread, (SETS,), (DMA((4,)),), at, a, ins=[ANY], to=ANY)
    near = exchange(copies, "y")
    a1 = shift(a, Z, -1)
    a3 = shift(a, Z, 1)
    a2 = lax.ppermute(a, Z, [(k, (k + (2 if k % 2 else -2)) % 16) for k in range(16)])
    (others,) = call(turn, ((3, 4, 96, 352),), (DMA((3,)),), at, near, ins=[ANY], to=ANY)
    z1 = shift(others, Z, -1)
    z3 = shift(others, Z, 1)
    (copies,) = call(spread, (SETS,), (DMA((4,)),), at, a2, ins=[ANY], to=ANY)
    far = exchange(copies, "y")
    pieces = (near, a1, a3, far, z1, z3)
    b0, b1, b2, b3 = call(columns, (COL,) * 4, ((4, *COL),), at, bt, gain)
    (tok,) = call(tokens, ((3, *TOK),), (), at, bt, ft, og, gain)
    b1 = shift(b1, "y", 1)
    b2 = shift(b2, "y", 2)
    b3 = shift(b3, "y", 3)
    (cols,) = call(merge, ((512, 512),), (), at, b0, b1, b2, b3)
    gds, keep, give = call(
        products,
        ((4, 4, 32, 352), (64, 4096), (64, 4096)),
        (W, W, W, (4, 32, 352), (128, 4096), DMA((3,)), DMA((8,))),
        at, tok, *pieces,
        ins=[VM] + [ANY] * 6,
        to=ANY,
    )
    gds = exchange(gds, "y")
    (grads,) = call(outer, ((16, 32, 352),), (), at, cols, gds)
    gz = exchange(grads, Z)
    other = shift(give, "c", 1)
    p0, p1, p2, p3 = call(pair, ((16, 4096),) * 4, (), at, keep, other)
    p1 = shift(p1, "x", 1)
    p2 = shift(p2, "x", 2)
    p3 = shift(p3, "x", -1)
    (done,) = call(finish, ((16, 4096),), (), at, p0, p1, p2, p3, bt, gain)
    half = lax.all_gather(done, "x", axis=0, tiled=True)
    other = shift(half, "c", 1)
    first = jnp.where(c == 0, half, other)
    second = jnp.where(c == 0, other, half)
    whole = jnp.concatenate([first, second], axis=0)
    grad = gsum + gz.astype(F32).sum(axis=0)
    return whole[:, :2048], whole[:, 2048:], grad


def solution(mesh):
    split = Mesh(mesh.devices.reshape(4, 4, 4, 4, 2), ("za", "zb", "y", "x", "c"))
    tok = P(FS, None)
    w = P(FS, TP)
    return jax.shard_map(
        shards,
        mesh=split,
        in_specs=(tok, tok, tok, P(), w, w, w, w),
        out_specs=(tok, tok, w),
        check_vma=False,
    )
```
